512 devices in a mesh: gr: 2 (over z_hi), fs: 32 (over z_lo, y), tp: 8 (over x, core).
Axes of the slice: x: 4, y: 4, z: 16 (z_hi: 2, z_lo: 8; z = z_hi * 8 + z_lo), core: 2. Of those that a mesh axis runs over, the one named last changes fastest.
Arguments:
- tokens: bfloat16 [8192, 2048], P(('gr', 'tp')), may hold values from -6 to 6
- norm_gain: float32 [2048], P('fs'), may hold values from 0.1 to 1.9
- up_weight: float32 [2048, 8192], P('fs', ('gr', 'tp')), may hold values from -0.125 to 0.125
- down_weight: float32 [8192, 2048], P('fs', ('gr', 'tp')), may hold values from -0.125 to 0.125
Outputs:
- sampler_up: bfloat16 [2048, 8192], P(None, 'fs')
- sampler_down: bfloat16 [8192, 2048], P('fs')
- mixed: bfloat16 [8192, 2048], P(('gr', 'tp'), 'fs')
The draws below stay inside these ranges and needn't reach their ends.
All inputs are finite; a program needn't handle non-finite values.
Results may differ from the reference program's by a relative error of at most 0.023.
Values may be sent and summed in bfloat16 or wider, within the bound.
A program may use at most 64 MiB of HBM per device.

```python
import jax
import jax.numpy as jnp
from jax import lax

D = 2048
FF = 8192
ROWS = 8192
N_FS = 32


def spiked(drawn, stream_key, source, target, blocks, factor):
    owner, partner = [(jnp.arange(drawn.shape[position]) // (drawn.shape[position] // blocks)).reshape([-1 if axis == position else 1 for axis in range(drawn.ndim)]) for position in (source, target)]
    chosen = jax.random.permutation(stream_key, blocks)[partner]
    strong = (owner == chosen) | (owner == (partner + blocks // 2) % blocks)
    return jnp.where(strong, factor * drawn, drawn)


def block_levels(rng, shape, cuts, smallest, top_value):
    gain, own = 1.0, jax.random.fold_in(rng, 6)
    for axis_at, blocks in cuts:
        draws = jnp.exp(jax.random.uniform(jax.random.fold_in(own, axis_at), (blocks,), jnp.float32, smallest / len(cuts), top_value / len(cuts)))
        gain = gain * jnp.repeat(draws, shape[axis_at] // blocks).reshape([-1 if axis == axis_at else 1 for axis in range(len(shape))])
    return gain


def bell_draw(key, extent, deviation, bound, cuts=(), held_as=jnp.bfloat16):
    result = jax.random.normal(key, extent, jnp.float32) * deviation
    if len(cuts) > 0:
        result = block_levels(key, extent, cuts, -0.22, 0.18) * result
    return jnp.clip(result, min=-bound, max=bound).astype(held_as)


def heavy_noise(own_key, dims, spread, limit, shards, heavy, held_as=jnp.bfloat16):
    entries = spread * jax.random.normal(own_key, dims, jnp.float32)
    if shards:
        entries = entries * block_levels(own_key, dims, shards, -0.22, 0.18)
    return jnp.clip(spiked(entries, jax.random.fold_in(own_key, 3), *heavy), -limit, limit).astype(held_as)


def setup_inputs(seed: int = 0) -> dict:
    streams_of = jax.random.split(jax.random.key(seed), 5)
    tokens = bell_draw(streams_of[0], (ROWS, D), 1.0, 6.0, ((0, 16),))
    norm_gain = jnp.clip(1.0 + 0.18 * jax.random.normal(streams_of[1], (D,), jnp.float32), 0.1, 1.9)
    up_weight = bell_draw(streams_of[2], (D, FF), D ** -0.5, 0.125, ((0, 32), (1, 16)), jnp.float32)
    down_weight = heavy_noise(streams_of[3], (FF, D), FF ** -0.5, 0.125, ((0, 32), (1, 16)), (0, 1, 32, 2.75), jnp.float32)
    return dict(tokens=tokens, norm_gain=norm_gain, up_weight=up_weight, down_weight=down_weight)


def reference(tokens, norm_gain, up_weight, down_weight):
    sampler_up = (norm_gain[:, None] * up_weight).astype(jnp.bfloat16)
    sampler_down = down_weight.astype(jnp.bfloat16)
    widened = tokens.astype(jnp.float32)
    normed = (widened * lax.rsqrt(lax.optimization_barrier(jnp.mean(widened * widened, axis=-1, keepdims=True)) + 1e-06)).astype(jnp.bfloat16)
    preact = jnp.dot(normed, sampler_up, preferred_element_type=jnp.float32)
    hidden = jnp.square(jax.nn.relu(preact)).astype(jnp.bfloat16)
    block_units = FF // N_FS

    def add_block(total, index):
        begin = (index * block_units).astype(jnp.int32)
        hidden_part = lax.dynamic_slice_in_dim(hidden, begin, block_units, 1)
        down_part = lax.dynamic_slice_in_dim(sampler_down, begin, block_units, 0)
        partial_value = jnp.dot(hidden_part, down_part, preferred_element_type=jnp.float32).astype(jnp.bfloat16)
        partial_value = lax.optimization_barrier(partial_value)
        return (total + partial_value.astype(jnp.float32), None)
    start_total = jnp.zeros((tokens.shape[0], D), jnp.float32)
    summed, _ = lax.scan(add_block, start_total, jnp.arange(N_FS, dtype=jnp.int32))
    return (sampler_up, sampler_down, summed.astype(jnp.bfloat16))
```

```python
import functools

import jax
import jax.numpy as jnp
from jax import lax
from jax.experimental import pallas as pl
from jax.experimental.pallas import tpu as pltpu
from jax.sharding import PartitionSpec as P

MESH = pl.DeviceIdType.MESH
F32 = jnp.float32
BF16 = jnp.bfloat16

TOK = 512
D = 2048
UNITS = 256
NT = 2
TC = TOK // NT

UP1 = 0
UPX1 = 4
UPX2 = 8
UPC = 10
DNG = 18
DNX1 = 19
DNX2 = 23
DNC = 25
DTY = 33
DTX1 = 37
DTX2 = 39
DTC = 41
HY1 = 46
HY2 = HY1 + 2 * NT
RS = HY2 + 2 * NT
N_MSG = RS + 3 * NT


def kernel(
    tok_hbm, gain_ref, upw_ref, dnw_ref,
    up_out, dn_out, mix_ref,
    u_send, up_buf, dn_buf, dt_send, dt_buf, nrm, h_buf,
    s1, r1, k1, s2, r2, k2, s3, r3, k3,
    ssem, rsem, lsem,
):
    g = lax.axis_index("gr")
    f = lax.axis_index("fs")
    t = lax.axis_index("tp")
    zl, y = f // 4, f % 4
    x, k = t // 2, t % 2
    ok = 1 - k
    og = 1 - g

    def dev(gg, zz, yy, xx, kk):
        return (gg, zz * 4 + yy, xx * 2 + kk)

    def send(src, dst, i, to, j=None):
        copy = pltpu.make_async_remote_copy(
            src_ref=src, dst_ref=dst,
            send_sem=ssem.at[i], recv_sem=rsem.at[i if j is None else j],
            device_id=to, device_id_type=MESH,
        )
        copy.start()
        return copy

    def arrived(dst, i):
        pltpu.make_async_remote_copy(
            src_ref=dst, dst_ref=dst,
            send_sem=ssem.at[0], recv_sem=rsem.at[i],
            device_id=dev(g, zl, y, x, ok), device_id_type=MESH,
        ).wait_recv()

    right, left, far = (x + 1) % 4, (x + 3) % 4, (x + 2) % 4
    to_right, to_left = dev(g, zl, y, right, k), dev(g, zl, y, left, k)
    to_core = dev(g, zl, y, x, ok)
    y_up, y_down, y_far = (y + 1) % 4, (y + 3) % 4, (y + 2) % 4
    to_yup, to_ydown = dev(g, zl, y_up, x, k), dev(g, zl, y_down, x, k)
    b0, b1, b2 = zl % 2, (zl // 2) % 2, zl // 4
    z1 = zl + 1 - 2 * b0
    z2 = zl + 2 - 4 * b1
    z4 = zl + 4 - 8 * b2

    xs, ks, hs = zl % 4, y // 2, y % 2

    def a_of(xx):
        return (xx - xs - hs - 2 * g + 8) % 4

    a_me = a_of(x)
    sources = [
        (q * 2 + w, dev(b2, a_me + 4 * q, 2 * ok + w, xs, ks)) for q in range(2) for w in range(2)
    ]

    barrier = pltpu.get_barrier_semaphore()
    greet = [s for _, s in sources] + [
        dev(og, zl, y, x, k), to_right, to_left, to_core,
        to_yup, to_ydown, dev(g, zl, y_far, x, k),
        dev(g, z1, y, x, k), dev(g, z2, y, x, k), dev(g, z4, y, x, k),
    ]
    for who in greet:
        pl.semaphore_signal(barrier, inc=1, device_id=who, device_id_type=MESH)

    tok_copy = pltpu.make_async_copy(tok_hbm, nrm, lsem.at[0])
    tok_copy.start()

    rows = lax.broadcasted_iota(jnp.int32, (64, 64), 0)
    cols = lax.broadcasted_iota(jnp.int32, (64, 64), 1)
    gain_wide = jnp.broadcast_to(gain_ref[...], (64, 64))
    gain = jnp.sum(jnp.where(rows == cols, gain_wide, 0.0), axis=1, keepdims=True)
    for h in range(2):
        u_send[h] = (gain * upw_ref[:, h * 256 : (h + 1) * 256]).astype(BF16)

    def dn_cols(gg, xx, kk):
        return pl.ds(pl.multiple_of((gg * 8 + xx * 2 + kk) * 128, 128), 128)

    def dn_piece(gg, xx, kk):
        return dn_buf.at[:, dn_cols(gg, xx, kk)]

    dn_mine = dnw_ref[...]
    dn_buf[:, dn_cols(g, x, k)] = dn_mine.astype(BF16)

    pl.semaphore_wait(barrier, len(greet))

    def up_piece(xx, q, kk):
        start = ((a_of(xx) + 4 * q) * 4 + 2 * (1 - kk)) * 64
        return up_buf.at[pl.ds(pl.multiple_of(start, 128), 128), :]

    sent = []
    j_me = (zl // 4) * 2 + y % 2
    for gg in range(2):
        for h in range(2):
            xx = (x + zl + h + 2 * gg) % 4
            to = (gg, (4 * g + x) * 4 + 2 * k + h, xx * 2 + (1 - y // 2))
            slot = up_buf.at[pl.ds(pl.multiple_of(f * 64, 64), 64), :]
            sent.append(send(u_send.at[h], slot, UP1 + gg * 2 + h, to, UP1 + j_me))
    sent.append(send(dn_piece(g, x, k), dn_piece(g, x, k), DNG, dev(og, zl, y, x, k)))

    dt_mine = dn_mine.T.astype(BF16)
    for h in range(2):
        dt_send[h, pl.ds(pl.multiple_of(g * 64, 64), 64), :] = dt_mine[h * 64 : (h + 1) * 64]

    tok_copy.wait()

    def norm_rows(i, _):
        at = pl.ds(pl.multiple_of(i * 16, 16), 16)
        wide = nrm[at, :].astype(F32)
        scale = lax.rsqrt(jnp.mean(wide * wide, axis=-1, keepdims=True) + 1e-06)
        nrm[at, :] = (wide * scale).astype(BF16)
        return 0

    lax.fori_loop(0, TOK // 16, norm_rows, 0)

    for j, _ in sources:
        q, w = j // 2, j % 2
        start = ((a_me + 4 * q) * 4 + 2 * ok + w) * 64
        arrived(up_buf.at[pl.ds(pl.multiple_of(start, 64), 64), :], UP1 + j)
        if w == 1:
            piece = up_piece(x, q, k)
            sent.append(send(piece, piece, UPX1 + q, to_right))
            sent.append(send(piece, piece, UPX1 + 2 + q, to_left))
            sent.append(send(piece, piece, UPC + q, to_core))

    arrived(dn_piece(og, x, k), DNG)
    for q in range(2):
        piece = dn_piece(q, x, k)
        sent.append(send(piece, piece, DNX1 + q, to_right))
        sent.append(send(piece, piece, DNX1 + 2 + q, to_left))
        sent.append(send(piece, piece, DNC + q, to_core))

    def dt_rows(xx, start=0, size=128):
        at = ((xx % 2) * 4 + (xx // 2) * 2) * 64 + start
        return pl.ds(pl.multiple_of(at, 64), size)

    dt_other = dn_buf[:, dn_cols(og, x, k)].astype(F32).T.astype(BF16)
    for h in range(2):
        dt_send[h, pl.ds(pl.multiple_of(og * 64, 64), 64), :] = dt_other[h * 64 : (h + 1) * 64]
    for h in range(2):
        target = 2 * k + h

        def dt_copy(h=h, target=target):
            return pltpu.make_async_remote_copy(
                src_ref=dt_send.at[h], dst_ref=dt_buf.at[y, dt_rows(x), :],
                send_sem=ssem.at[DTY + h], recv_sem=rsem.at[DTY + y],
                device_id=dev(g, zl, target, x, k), device_id_type=MESH,
            )

        @pl.when(target != y)
        def _():
            dt_copy().start()

        @pl.when(target == y)
        def _():
            dt_buf[y, dt_rows(x), :] = dt_send[h]

    for q in range(2):
        piece = up_piece(left, q, k)
        arrived(piece, UPX1 + q)
        if q == 0:
            sent.append(send(piece, piece, UPX2, to_right))
        sent.append(send(piece, piece, UPC + 2 + q, to_core))
        piece = up_piece(right, q, k)
        arrived(piece, UPX1 + 2 + q)
        if q == 1:
            sent.append(send(piece, piece, UPX2 + 1, to_left))
        sent.append(send(piece, piece, UPC + 4 + q, to_core))
    for q in range(2):
        piece = up_piece(far, q, k)
        arrived(piece, UPX2 + q)
        sent.append(send(piece, piece, UPC + 6 + q, to_core))

    def dn_forward():
        for q in range(2):
            piece = dn_piece(q, left, k)
            arrived(piece, DNX1 + q)
            if q == 0:
                sent.append(send(piece, piece, DNX2, to_right))
            sent.append(send(piece, piece, DNC + 2 + q, to_core))
            piece = dn_piece(q, right, k)
            arrived(piece, DNX1 + 2 + q)
            if q == 1:
                sent.append(send(piece, piece, DNX2 + 1, to_left))
            sent.append(send(piece, piece, DNC + 4 + q, to_core))

    dn_forward()

    owner = ks == k

    def dt_piece(xx, start=0, size=128):
        return dt_buf.at[:, dt_rows(xx, start, size), :]

    def dt_msg(piece, i, to):
        return pltpu.make_async_remote_copy(
            src_ref=piece, dst_ref=piece, send_sem=ssem.at[i], recv_sem=rsem.at[i],
            device_id=to, device_id_type=MESH,
        )

    @pl.when(owner)
    def _():
        for src in range(4):

            @pl.when(y != src)
            def _():
                arrived(dt_buf.at[src, dt_rows(x), :], DTY + src)

        dt_msg(dt_piece(x), DTX1, to_right).start()
        dt_msg(dt_piece(x), DTX1 + 1, to_left).start()
        dt_msg(dt_piece(x), DTC, to_core).start()

    for i, xx in enumerate((x, left, right, far)):
        for q in range(2):
            arrived(up_piece(xx, q, ok), UPC + 2 * i + q)
    up_copy = pltpu.make_async_copy(up_buf, up_out, lsem.at[1])
    up_copy.start()
    for j in range(NT):
        at = pl.ds(j * TC, TC)
        pre = jnp.dot(nrm[at, :], up_buf[...], preferred_element_type=F32)
        pre = jnp.maximum(pre, 0.0)
        h_buf[y, at, :] = (pre * pre).astype(BF16)
        piece = h_buf.at[y, at, :]
        sent.append(send(piece, piece, HY1 + 2 * j, to_yup))
        sent.append(send(piece, piece, HY1 + 2 * j + 1, to_ydown))

    @pl.when(owner)
    def _():
        arrived(dt_piece(left), DTX1)
        dt_msg(dt_piece(left, 0, 64), DTX2, to_right).start()
        dt_msg(dt_piece(left), DTC + 1, to_core).start()
        arrived(dt_piece(right), DTX1 + 1)
        dt_msg(dt_piece(right, 64, 64), DTX2 + 1, to_left).start()
        dt_msg(dt_piece(right), DTC + 2, to_core).start()

    for q in range(2):
        piece = dn_piece(q, far, k)
        arrived(piece, DNX2 + q)
        sent.append(send(piece, piece, DNC + 6 + q, to_core))

    half = TC // 2
    for j in range(NT):
        low, high = pl.ds(j * TC, half), pl.ds(j * TC + half, half)
        at = pl.ds(j * TC, TC)
        arrived(h_buf.at[y_down, at, :], HY1 + 2 * j)
        piece = h_buf.at[y_down, low, :]
        sent.append(send(piece, piece, HY2 + 2 * j, to_yup))
        arrived(h_buf.at[y_up, at, :], HY1 + 2 * j + 1)
        piece = h_buf.at[y_up, high, :]
        sent.append(send(piece, piece, HY2 + 2 * j + 1, to_ydown))

    @pl.when(owner)
    def _():
        for q in range(2):
            arrived(dt_piece(far, 64 * q, 64), DTX2 + q)
            dt_msg(dt_piece(far, 64 * q, 64), DTC + 3 + q, to_core).start()

    @pl.when(jnp.logical_not(owner))
    def _():
        arrived(dt_piece(x), DTC)
        arrived(dt_piece(left), DTC + 1)
        arrived(dt_piece(right), DTC + 2)
        for q in range(2):
            arrived(dt_piece(far, 64 * q, 64), DTC + 3 + q)

    def times_hidden(rows_at, size, at):
        total = jnp.zeros((size, TC), F32)
        for yy in range(4):
            total += lax.dot_general(
                dt_buf[yy, rows_at, :], h_buf[yy, at, :],
                (((1,), (1,)), ((), ())), preferred_element_type=F32,
            )
        return total

    def aligned(start, size):
        return pl.ds(pl.multiple_of(start, 64), size)

    to_z1, to_z2, to_z4 = (dev(g, zz, y, x, k) for zz in (z1, z2, z4))
    for j in range(NT):
        at = pl.ds(j * TC, TC)
        low, high = pl.ds(j * TC, half), pl.ds(j * TC + half, half)
        arrived(h_buf.at[y_far, low, :], HY2 + 2 * j)
        arrived(h_buf.at[y_far, high, :], HY2 + 2 * j + 1)
        s1[j] = times_hidden(aligned((1 - b0) * 256, 256), 256, at).astype(BF16)
        sent.append(send(s1.at[j], r1.at[j], RS + 3 * j, to_z1))
        k1[j] = times_hidden(aligned(b0 * 256, 256), 256, at)

    for j in range(NT):
        arrived(r1.at[j], RS + 3 * j)
        out, keep = aligned((1 - b1) * 128, 128), aligned(b1 * 128, 128)
        s2[j] = (k1[j, out, :] + r1[j, out, :].astype(F32)).astype(BF16)
        sent.append(send(s2.at[j], r2.at[j], RS + 3 * j + 1, to_z2))
        k2[j] = k1[j, keep, :] + r1[j, keep, :].astype(F32)
    for j in range(NT):
        arrived(r2.at[j], RS + 3 * j + 1)
        out, keep = aligned((1 - b2) * 64, 64), aligned(b2 * 64, 64)
        s3[j] = (k2[j, out, :] + r2[j, out, :].astype(F32)).astype(BF16)
        sent.append(send(s3.at[j], r3.at[j], RS + 3 * j + 2, to_z4))
        k3[j] = k2[j, keep, :] + r2[j, keep, :].astype(F32)

    for i, xx in enumerate((x, left, right, far)):
        for q in range(2):
            arrived(dn_piece(q, xx, ok), DNC + 2 * i + q)
    dn_copy = pltpu.make_async_copy(dn_buf, dn_out, lsem.at[2])
    dn_copy.start()

    for j in range(NT):
        arrived(r3.at[j], RS + 3 * j + 2)
        mix_ref[:, j * TC : (j + 1) * TC] = (k3[j] + r3[j].astype(F32)).astype(BF16)

    for copy in sent:
        copy.wait_send()
    for h in range(2):

        @pl.when(2 * k + h != y)
        def _():
            pltpu.make_async_remote_copy(
                src_ref=dt_send.at[h], dst_ref=dt_send.at[h],
                send_sem=ssem.at[DTY + h], recv_sem=rsem.at[DTY],
                device_id=to_core, device_id_type=MESH,
            ).wait_send()

    @pl.when(owner)
    def _():
        dt_msg(dt_piece(x), DTX1, to_right).wait_send()
        dt_msg(dt_piece(x), DTX1 + 1, to_left).wait_send()
        dt_msg(dt_piece(x), DTC, to_core).wait_send()
        dt_msg(dt_piece(left, 0, 64), DTX2, to_right).wait_send()
        dt_msg(dt_piece(left), DTC + 1, to_core).wait_send()
        dt_msg(dt_piece(right, 64, 64), DTX2 + 1, to_left).wait_send()
        dt_msg(dt_piece(right), DTC + 2, to_core).wait_send()
        for q in range(2):
            dt_msg(dt_piece(far, 64 * q, 64), DTC + 3 + q, to_core).wait_send()

    up_copy.wait()
    dn_copy.wait()


def per_device(tokens, norm_gain, up_weight, down_weight):
    vmem = pl.BlockSpec(memory_space=pltpu.VMEM)
    anywhere = pl.BlockSpec(memory_space=pl.ANY)
    up_block, down_block, mixed = pl.pallas_call(
        kernel,
        out_shape=(
            jax.ShapeDtypeStruct((D, UNITS), BF16),
            jax.ShapeDtypeStruct((UNITS, D), BF16),
            jax.ShapeDtypeStruct((64, TOK), BF16),
        ),
        in_specs=[anywhere, vmem, vmem, vmem],
        out_specs=(anywhere, anywhere, vmem),
        scratch_shapes=[
            pltpu.VMEM((2, 64, 256), BF16),
            pltpu.VMEM((D, UNITS), BF16),
            pltpu.VMEM((UNITS, D), BF16),
            pltpu.VMEM((2, 128, 256), BF16),
            pltpu.VMEM((4, 512, 256), BF16),
            pltpu.VMEM((TOK, D), BF16),
            pltpu.VMEM((4, TOK, UNITS), BF16),
            pltpu.VMEM((NT, 256, TC), BF16),
            pltpu.VMEM((NT, 256, TC), BF16),
            pltpu.VMEM((NT, 256, TC), F32),
            pltpu.VMEM((NT, 128, TC), BF16),
            pltpu.VMEM((NT, 128, TC), BF16),
            pltpu.VMEM((NT, 128, TC), F32),
            pltpu.VMEM((NT, 64, TC), BF16),
            pltpu.VMEM((NT, 64, TC), BF16),
            pltpu.VMEM((NT, 64, TC), F32),
            pltpu.SemaphoreType.DMA((N_MSG,)),
            pltpu.SemaphoreType.DMA((N_MSG,)),
            pltpu.SemaphoreType.DMA((3,)),
        ],
        compiler_params=pltpu.CompilerParams(
            collective_id=0, has_side_effects=True, vmem_limit_bytes=40 * 1024 * 1024
        ),
        name="handoff",
    )(tokens, norm_gain.reshape(1, 64), up_weight, down_weight)
    return up_block, down_block, mixed.T


def solution(mesh):
    in_specs = (P(("gr", "tp"), None), P("fs"), P("fs", ("gr", "tp")), P("fs", ("gr", "tp")))
    out_specs = (P(None, "fs"), P("fs", None), P(("gr", "tp"), "fs"))
    return jax.shard_map(
        per_device, mesh=mesh, in_specs=in_specs, out_specs=out_specs, check_vma=False
    )
```

```python
import jax
import jax.numpy as jnp
from jax import lax
from jax.experimental import pallas as pl
from jax.experimental.pallas import tpu as pltpu
from jax.sharding import PartitionSpec as P

MESH = pl.DeviceIdType.MESH
F32 = jnp.float32
BF16 = jnp.bfloat16

TOK = 512
D = 2048
UNITS = 256
HALF = 128
NT = 4
TC = TOK // NT
H_CHUNKS = ((0, 2, 256), (1, NT, TC))


def numbered(*sizes):
    firsts, at = [], 0
    for size in sizes:
        firsts.append(at)
        at += size
    return (*firsts, at)


UP1, UPX, UPC, DNG, DNX, DNC, DTY, DTX, DTC, HY, RS, N_MSG = numbered(
    8, 12, 16, 1, 6, 8, 4, 3, 4, 6 + 3 * NT, 3 * NT
)


def kernel(
    tok_hbm, gain_hbm, upw_hbm, dnw_hbm,
    up_out, dn_out, mix_ref,
    gain_ref, upw_ref, dnw_ref,
    u_send, up_buf, dn_buf, dt_send, dt_buf, nrm, h_buf,
    s1, r1, k1, s2, r2, k2, s3, r3, k3,
    ssem, rsem, lsem,
):
    g = lax.axis_index("gr")
    f = lax.axis_index("fs")
    t = lax.axis_index("tp")
    zl, y = f // 4, f % 4
    x, k = t // 2, t % 2
    ok = 1 - k
    og = 1 - g

    def dev(gg, zz, yy, xx, kk):
        return (gg, zz * 4 + yy, xx * 2 + kk)

    def message(src, dst, i, to, j=None):
        return pltpu.make_async_remote_copy(
            src_ref=src, dst_ref=dst,
            send_sem=ssem.at[i], recv_sem=rsem.at[i if j is None else j],
            device_id=to, device_id_type=MESH,
        )

    sent = []

    def send(src, dst, i, to, j=None):
        copy = message(src, dst, i, to, j)
        copy.start()
        sent.append(copy)

    to_core = dev(g, zl, y, x, ok)

    def arrived(dst, i):
        message(dst, dst, 0, to_core, i).wait_recv()

    steps = (2, 1, 3)
    x_to = [dev(g, zl, y, (x + s) % 4, k) for s in steps]
    x_from = [(x + 4 - s) % 4 for s in steps]
    y_to = [dev(g, zl, (y + s) % 4, x, k) for s in steps]
    y_from = [(y + 4 - s) % 4 for s in steps]
    b0, b1, b2 = zl % 2, (zl // 2) % 2, zl // 4
    to_z1 = dev(g, zl + 1 - 2 * b0, y, x, k)
    to_z2 = dev(g, zl + 2 - 4 * b1, y, x, k)
    to_z4 = dev(g, zl + 4 - 8 * b2, y, x, k)
    to_gr = dev(og, zl, y, x, k)

    xs, ks, hs = zl % 4, y // 2, y % 2

    def a_of(xx):
        return (xx - xs - hs - 2 * g + 8) % 4

    a_me = a_of(x)
    sources = [
        (q * 2 + w, dev(b2, a_me + 4 * q, 2 * ok + w, xs, ks)) for q in range(2) for w in range(2)
    ]

    barrier = pltpu.get_barrier_semaphore()
    greet = [s for _, s in sources] + [to_gr, *x_to, *y_to, to_z1, to_z2, to_z4, to_core]
    for who in greet:
        pl.semaphore_signal(barrier, inc=1, device_id=who, device_id_type=MESH)

    loads = [
        pltpu.make_async_copy(src, dst, lsem.at[i])
        for i, (src, dst) in enumerate(
            ((gain_hbm, gain_ref), (upw_hbm, upw_ref), (dnw_hbm, dnw_ref), (tok_hbm, nrm))
        )
    ]
    for load in loads:
        load.start()

    loads[0].wait()
    loads[1].wait()
    rows = lax.broadcasted_iota(jnp.int32, (64, 64), 0)
    cols = lax.broadcasted_iota(jnp.int32, (64, 64), 1)
    gain_wide = jnp.broadcast_to(gain_ref[...], (64, 64))
    gain = jnp.sum(jnp.where(rows == cols, gain_wide, 0.0), axis=1, keepdims=True)
    for h in range(2):
        u_send[h] = (gain * upw_ref[:, h * 256 : (h + 1) * 256]).astype(BF16)

    def dn_cols(gg, xx, kk):
        return pl.ds(pl.multiple_of((gg * 8 + xx * 2 + kk) * 128, 128), 128)

    def dn_piece(gg, xx, kk):
        return dn_buf.at[:, dn_cols(gg, xx, kk)]

    loads[2].wait()
    dn_mine = dnw_ref[...]
    dn_buf[:, dn_cols(g, x, k)] = dn_mine.astype(BF16)

    dt_mine = dn_mine.T.astype(BF16)
    for h in range(2):
        dt_send[h, pl.ds(pl.multiple_of(g * 64, 64), 64), :] = dt_mine[h * 64 : (h + 1) * 64]

    pl.semaphore_wait(barrier, len(greet))

    def up_piece(xx, q, kk, u):
        start = ((a_of(xx) + 4 * q) * 4 + 2 * (1 - kk)) * 64
        return up_buf.at[pl.ds(pl.multiple_of(start, 128), 128), pl.ds(u * HALF, HALF)]

    j_me = b2 * 2 + y % 2
    for u in range(2):
        for gg in range(2):
            for h in range(2):
                xx = (x + zl + h + 2 * gg) % 4
                to = (gg, (4 * g + x) * 4 + 2 * k + h, xx * 2 + (1 - y // 2))
                slot = up_buf.at[pl.ds(pl.multiple_of(f * 64, 64), 64), pl.ds(u * HALF, HALF)]
                src = u_send.at[h, :, pl.ds(u * HALF, HALF)]
                send(src, slot, UP1 + u * 4 + gg * 2 + h, to, UP1 + u * 4 + j_me)

    loads[3].wait()

    def norm_rows(i, _):
        at = pl.ds(pl.multiple_of(i * 16, 16), 16)
        wide = nrm[at, :].astype(F32)
        scale = lax.rsqrt(jnp.mean(wide * wide, axis=-1, keepdims=True) + 1e-06)
        nrm[at, :] = (wide * scale).astype(BF16)
        return 0

    lax.fori_loop(0, TOK // 32, norm_rows, 0)
    send(dn_piece(g, x, k), dn_piece(g, x, k), DNG, to_gr)
    lax.fori_loop(TOK // 32, TOK // 16, norm_rows, 0)

    for u in range(2):
        for j, _ in sources:
            q, w = j // 2, j % 2
            start = ((a_me + 4 * q) * 4 + 2 * ok + w) * 64
            slot = up_buf.at[pl.ds(pl.multiple_of(start, 64), 64), pl.ds(u * HALF, HALF)]
            arrived(slot, UP1 + u * 4 + j)
            if w == 1:
                piece = up_piece(x, q, k, u)
                for d in range(3):
                    send(piece, piece, UPX + u * 6 + q * 3 + d, x_to[d])
                send(piece, piece, UPC + u * 8 + q * 4, to_core)

    def up_to_core(u):
        for d in (1, 2, 0):
            for q in range(2):
                piece = up_piece(x_from[d], q, k, u)
                arrived(piece, UPX + u * 6 + q * 3 + d)
                send(piece, piece, UPC + u * 8 + q * 4 + 1 + d, to_core)

    def hidden_half(u):
        for q in range(2):
            arrived(up_piece(x, q, ok, u), UPC + u * 8 + q * 4)
            for d in range(3):
                arrived(up_piece(x_from[d], q, ok, u), UPC + u * 8 + q * 4 + 1 + d)
        _, count, size = H_CHUNKS[u]
        units = pl.ds(u * HALF, HALF)
        for part in range(2):
            at = pl.ds(part * 256, 256)
            pre = jnp.dot(nrm[at, :], up_buf[:, units], preferred_element_type=F32)
            pre = jnp.maximum(pre, 0.0)
            h_buf[y, at, units] = (pre * pre).astype(BF16)
            for j in range(part * count // 2, (part + 1) * count // 2):
                piece = h_buf.at[y, pl.ds(j * size, size), units]
                for d in range(3):
                    send(piece, piece, HY + u * 6 + j * 3 + d, y_to[d])

    up_to_core(0)
    hidden_half(0)

    arrived(dn_piece(og, x, k), DNG)

    def dt_rows(xx):
        return pl.ds(pl.multiple_of(((xx % 2) * 4 + (xx // 2) * 2) * 64, 128), 128)

    dt_other = dn_buf[:, dn_cols(og, x, k)].astype(F32).T.astype(BF16)
    for h in range(2):
        dt_send[h, pl.ds(pl.multiple_of(og * 64, 64), 64), :] = dt_other[h * 64 : (h + 1) * 64]

    def dt_to_y(h):
        return message(
            dt_send.at[h], dt_buf.at[y, dt_rows(x), :], DTY + h, dev(g, zl, 2 * k + h, x, k), DTY + y
        )

    for h in range(2):

        @pl.when(2 * k + h != y)
        def _():
            dt_to_y(h).start()

        @pl.when(2 * k + h == y)
        def _():
            dt_buf[y, dt_rows(x), :] = dt_send[h]

    for q in range(2):
        piece = dn_piece(q, x, k)
        for d in range(3):
            send(piece, piece, DNX + q * 3 + d, x_to[d])
        send(piece, piece, DNC + q * 4, to_core)

    up_to_core(1)
    hidden_half(1)
    up_copy = pltpu.make_async_copy(up_buf, up_out, lsem.at[0])
    up_copy.start()

    owner = ks == k

    def dt_piece(xx):
        return dt_buf.at[:, dt_rows(xx), :]

    def dt_along_x():
        return [message(dt_piece(x), dt_piece(x), DTX + d, x_to[d]) for d in range(3)] + [
            message(dt_piece(x), dt_piece(x), DTC, to_core)
        ]

    def dt_to_core(d):
        return message(dt_piece(x_from[d]), dt_piece(x_from[d]), DTC + 1 + d, to_core)

    @pl.when(owner)
    def _():
        for src in range(4):

            @pl.when(y != src)
            def _():
                arrived(dt_buf.at[src, dt_rows(x), :], DTY + src)

        for copy in dt_along_x():
            copy.start()

    for q in range(2):
        for d in (1, 2, 0):
            piece = dn_piece(q, x_from[d], k)
            arrived(piece, DNX + q * 3 + d)
            send(piece, piece, DNC + q * 4 + 1 + d, to_core)

    @pl.when(owner)
    def _():
        for d in (1, 2, 0):
            arrived(dt_piece(x_from[d]), DTX + d)
            dt_to_core(d).start()

    @pl.when(jnp.logical_not(owner))
    def _():
        arrived(dt_piece(x), DTC)
        for d in range(3):
            arrived(dt_piece(x_from[d]), DTC + 1 + d)

    def times_hidden(rows_at, size, at):
        total = jnp.zeros((size, TC), F32)
        for yy in range(4):
            total += lax.dot_general(
                dt_buf[yy, rows_at, :], h_buf[yy, at, :],
                (((1,), (1,)), ((), ())), preferred_element_type=F32,
            )
        return total

    def aligned(start, size):
        return pl.ds(pl.multiple_of(start, 64), size)

    def hidden_in(u, j):
        _, _, size = H_CHUNKS[u]
        for d in range(3):
            arrived(h_buf.at[y_from[d], pl.ds(j * size, size), pl.ds(u * HALF, HALF)], HY + u * 6 + j * 3 + d)

    for j in range(NT):
        at = pl.ds(j * TC, TC)
        if j % (NT // 2) == 0:
            hidden_in(0, j // (NT // 2))
        hidden_in(1, j)
        s1[j] = times_hidden(aligned((1 - b0) * 256, 256), 256, at).astype(BF16)
        send(s1.at[j], r1.at[j], RS + 3 * j, to_z1)
        k1[j] = times_hidden(aligned(b0 * 256, 256), 256, at)

    for j in range(NT):
        arrived(r1.at[j], RS + 3 * j)
        out, keep = aligned((1 - b1) * 128, 128), aligned(b1 * 128, 128)
        s2[j] = (k1[j, out, :] + r1[j, out, :].astype(F32)).astype(BF16)
        send(s2.at[j], r2.at[j], RS + 3 * j + 1, to_z2)
        k2[j] = k1[j, keep, :] + r1[j, keep, :].astype(F32)
    for j in range(NT):
        arrived(r2.at[j], RS + 3 * j + 1)
        out, keep = aligned((1 - b2) * 64, 64), aligned(b2 * 64, 64)
        s3[j] = (k2[j, out, :] + r2[j, out, :].astype(F32)).astype(BF16)
        send(s3.at[j], r3.at[j], RS + 3 * j + 2, to_z4)
        k3[j] = k2[j, keep, :] + r2[j, keep, :].astype(F32)

    for q in range(2):
        arrived(dn_piece(q, x, ok), DNC + q * 4)
        for d in range(3):
            arrived(dn_piece(q, x_from[d], ok), DNC + q * 4 + 1 + d)
    dn_copy = pltpu.make_async_copy(dn_buf, dn_out, lsem.at[1])
    dn_copy.start()

    for j in range(NT):
        arrived(r3.at[j], RS + 3 * j + 2)
        mix_ref[:, j * TC : (j + 1) * TC] = (k3[j] + r3[j].astype(F32)).astype(BF16)

    for copy in sent:
        copy.wait_send()
    for h in range(2):

        @pl.when(2 * k + h != y)
        def _():
            dt_to_y(h).wait_send()

    @pl.when(owner)
    def _():
        for copy in dt_along_x():
            copy.wait_send()
        for d in range(3):
            dt_to_core(d).wait_send()

    up_copy.wait()
    dn_copy.wait()


def per_device(tokens, norm_gain, up_weight, down_weight):
    hbm = pl.BlockSpec(memory_space=pltpu.HBM)
    vmem = pl.BlockSpec(memory_space=pltpu.VMEM)
    up_block, down_block, mixed = pl.pallas_call(
        kernel,
        out_shape=(
            jax.ShapeDtypeStruct((D, UNITS), BF16),
            jax.ShapeDtypeStruct((UNITS, D), BF16),
            jax.ShapeDtypeStruct((64, TOK), BF16),
        ),
        in_specs=[hbm] * 4,
        out_specs=(hbm, hbm, vmem),
        scratch_shapes=[
            pltpu.VMEM((1, 64), F32),
            pltpu.VMEM((64, 512), F32),
            pltpu.VMEM((256, 128), F32),
            pltpu.VMEM((2, 64, 256), BF16),
            pltpu.VMEM((D, UNITS), BF16),
            pltpu.VMEM((UNITS, D), BF16),
            pltpu.VMEM((2, 128, 256), BF16),
            pltpu.VMEM((4, 512, 256), BF16),
            pltpu.VMEM((TOK, D), BF16),
            pltpu.VMEM((4, TOK, UNITS), BF16),
            pltpu.VMEM((NT, 256, TC), BF16),
            pltpu.VMEM((NT, 256, TC), BF16),
            pltpu.VMEM((NT, 256, TC), F32),
            pltpu.VMEM((NT, 128, TC), BF16),
            pltpu.VMEM((NT, 128, TC), BF16),
            pltpu.VMEM((NT, 128, TC), F32),
            pltpu.VMEM((NT, 64, TC), BF16),
            pltpu.VMEM((NT, 64, TC), BF16),
            pltpu.VMEM((NT, 64, TC), F32),
            pltpu.SemaphoreType.DMA((N_MSG,)),
            pltpu.SemaphoreType.DMA((N_MSG,)),
            pltpu.SemaphoreType.DMA((4,)),
        ],
        compiler_params=pltpu.CompilerParams(
            collective_id=0, has_side_effects=True, vmem_limit_bytes=60 * 1024 * 1024
        ),
        name="handoff",
    )(tokens, norm_gain.reshape(1, 64), up_weight, down_weight)
    return up_block, down_block, mixed.T


def solution(mesh):
    in_specs = (P(("gr", "tp"), None), P("fs"), P("fs", ("gr", "tp")), P("fs", ("gr", "tp")))
    out_specs = (P(None, "fs"), P("fs", None), P(("gr", "tp"), "fs"))
    return jax.shard_map(
        per_device, mesh=mesh, in_specs=in_specs, out_specs=out_specs, check_vma=False
    )
```

```python
import jax
import jax.numpy as jnp
from jax import lax
from jax.experimental import pallas as pl
from jax.experimental.pallas import tpu as pltpu
from jax.sharding import PartitionSpec as P

MESH = pl.DeviceIdType.MESH
F32 = jnp.float32
BF16 = jnp.bfloat16

TOK = 512
D = 2048
UNITS = 256
HALF = 128
NT = 4
TC = TOK // NT
NORM_A, NORM_B = 20, 32
H_CHUNKS = ((0, 2, 256), (1, NT, TC))


def numbered(*sizes):
    firsts, at = [], 0
    for size in sizes:
        firsts.append(at)
        at += size
    return (*firsts, at)


UP1, UPX, UPC, DNG, DNX, DNC, DTY, DTX, DTC, HY, RS, N_MSG = numbered(
    8, 12, 16, 1, 6, 8, 8, 6, 8, 6 + 3 * NT, 3 * NT
)


def kernel(
    tok_hbm, gain_hbm, upw_hbm, dnw_hbm,
    up_buf, dn_buf, mix_ref,
    gain_ref, upw_ref, dnw_ref,
    u_send, dt_send, dt_buf, nrm, h_buf,
    s1, r1, k1, s2, r2, k2, s3, r3, k3,
    ssem, rsem, lsem,
):
    g = lax.axis_index("gr")
    f = lax.axis_index("fs")
    t = lax.axis_index("tp")
    zl, y = f // 4, f % 4
    x, k = t // 2, t % 2
    ok = 1 - k
    og = 1 - g

    def dev(gg, zz, yy, xx, kk):
        return (gg, zz * 4 + yy, xx * 2 + kk)

    def message(src, dst, i, to, j=None):
        return pltpu.make_async_remote_copy(
            src_ref=src, dst_ref=dst,
            send_sem=ssem.at[i], recv_sem=rsem.at[i if j is None else j],
            device_id=to, device_id_type=MESH,
        )

    sent = []

    def send(src, dst, i, to, j=None):
        copy = message(src, dst, i, to, j)
        copy.start()
        sent.append(copy)

    to_core = dev(g, zl, y, x, ok)

    def arrived(dst, i):
        message(dst, dst, 0, to_core, i).wait_recv()

    steps = (2, 1, 3)
    x_to = [dev(g, zl, y, (x + s) % 4, k) for s in steps]
    x_from = [(x + 4 - s) % 4 for s in steps]
    y_to = [dev(g, zl, (y + s) % 4, x, k) for s in steps]
    y_from = [(y + 4 - s) % 4 for s in steps]
    b0, b1, b2 = zl % 2, (zl // 2) % 2, zl // 4
    to_z1 = dev(g, zl + 1 - 2 * b0, y, x, k)
    to_z2 = dev(g, zl + 2 - 4 * b1, y, x, k)
    to_z4 = dev(g, zl + 4 - 8 * b2, y, x, k)
    to_gr = dev(og, zl, y, x, k)

    xs, ks, hs = zl % 4, y // 2, y % 2

    def a_of(xx):
        return (xx - xs - hs - 2 * g + 8) % 4

    a_me = a_of(x)
    sources = [
        (q * 2 + w, dev(b2, a_me + 4 * q, 2 * ok + w, xs, ks)) for q in range(2) for w in range(2)
    ]

    barrier = pltpu.get_barrier_semaphore()
    greet = [s for _, s in sources] + [to_gr, *x_to, *y_to, to_z1, to_z2, to_z4, to_core]
    for who in greet:
        pl.semaphore_signal(barrier, inc=1, device_id=who, device_id_type=MESH)

    loads = [
        pltpu.make_async_copy(src, dst, lsem.at[i])
        for i, (src, dst) in enumerate(
            ((gain_hbm, gain_ref), (upw_hbm, upw_ref), (dnw_hbm, dnw_ref), (tok_hbm, nrm))
        )
    ]
    for load in loads:
        load.start()

    loads[0].wait()
    loads[1].wait()
    rows = lax.broadcasted_iota(jnp.int32, (64, 64), 0)
    cols = lax.broadcasted_iota(jnp.int32, (64, 64), 1)
    gain_wide = jnp.broadcast_to(gain_ref[...], (64, 64))
    gain = jnp.sum(jnp.where(rows == cols, gain_wide, 0.0), axis=1, keepdims=True)
    for h in range(2):
        u_send[h] = (gain * upw_ref[:, h * 256 : (h + 1) * 256]).astype(BF16)

    def dn_cols(gg, xx, kk):
        return pl.ds(pl.multiple_of((gg * 8 + xx * 2 + kk) * 128, 128), 128)

    def dn_piece(gg, xx, kk):
        return dn_buf.at[:, dn_cols(gg, xx, kk)]

    loads[2].wait()
    dn_mine = dnw_ref[...]
    dn_buf[:, dn_cols(g, x, k)] = dn_mine.astype(BF16)

    dt_mine = dn_mine.T.astype(BF16)
    for h in range(2):
        dt_send[0, h] = dt_mine[h * 64 : (h + 1) * 64]

    pl.semaphore_wait(barrier, len(greet))

    def up_piece(xx, q, kk, u):
        start = ((a_of(xx) + 4 * q) * 4 + 2 * (1 - kk)) * 64
        return up_buf.at[pl.ds(pl.multiple_of(start, 128), 128), pl.ds(u * HALF, HALF)]

    j_me = b2 * 2 + y % 2
    for u in range(2):
        for gg in range(2):
            for h in range(2):
                xx = (x + zl + h + 2 * gg) % 4
                to = (gg, (4 * g + x) * 4 + 2 * k + h, xx * 2 + (1 - y // 2))
                slot = up_buf.at[pl.ds(pl.multiple_of(f * 64, 64), 64), pl.ds(u * HALF, HALF)]
                src = u_send.at[h, :, pl.ds(u * HALF, HALF)]
                send(src, slot, UP1 + u * 4 + gg * 2 + h, to, UP1 + u * 4 + j_me)

    owner = ks == k
    halves = (g, og)

    def dt_rows(part, xx):
        return pl.ds(pl.multiple_of(((xx % 2) * 4 + (xx // 2) * 2 + halves[part]) * 64, 64), 64)

    def dt_piece(part, xx):
        return dt_buf.at[:, dt_rows(part, xx), :]

    def dt_to_y(part, h):
        return message(
            dt_send.at[part, h], dt_buf.at[y, dt_rows(part, x), :],
            DTY + part * 4 + h, dev(g, zl, 2 * k + h, x, k), DTY + part * 4 + y,
        )

    def dt_over_y(part):
        for h in range(2):

            @pl.when(2 * k + h != y)
            def _():
                dt_to_y(part, h).start()

            @pl.when(2 * k + h == y)
            def _():
                dt_buf[y, dt_rows(part, x), :] = dt_send[part, h]

    def dt_from_x(part):
        piece = dt_piece(part, x)
        return [message(piece, piece, DTX + part * 3 + d, x_to[d]) for d in range(3)] + [
            message(piece, piece, DTC + part * 4, to_core)
        ]

    def dt_over_x(part):
        @pl.when(owner)
        def _():
            for src in range(4):

                @pl.when(y != src)
                def _():
                    arrived(dt_buf.at[src, dt_rows(part, x), :], DTY + part * 4 + src)

            for copy in dt_from_x(part):
                copy.start()

    def dt_to_core(part, d):
        piece = dt_piece(part, x_from[d])
        return message(piece, piece, DTC + part * 4 + 1 + d, to_core)

    def dt_over_core(part):
        @pl.when(owner)
        def _():
            for d in (1, 2, 0):
                arrived(dt_piece(part, x_from[d]), DTX + part * 3 + d)
                dt_to_core(part, d).start()

    def dn_over_x(part):
        piece = dn_piece(halves[part], x, k)
        for d in range(3):
            send(piece, piece, DNX + part * 3 + d, x_to[d])
        send(piece, piece, DNC + part * 4, to_core)

    def dn_over_core(part):
        for d in (1, 2, 0):
            piece = dn_piece(halves[part], x_from[d], k)
            arrived(piece, DNX + part * 3 + d)
            send(piece, piece, DNC + part * 4 + 1 + d, to_core)

    dt_over_y(0)
    dn_over_x(0)

    loads[3].wait()

    def norm_rows(i, _):
        at = pl.ds(pl.multiple_of(i * 16, 16), 16)
        wide = nrm[at, :].astype(F32)
        scale = lax.rsqrt(jnp.mean(wide * wide, axis=-1, keepdims=True) + 1e-06)
        nrm[at, :] = (wide * scale).astype(BF16)
        return 0

    lax.fori_loop(0, NORM_A, norm_rows, 0)
    dt_over_x(0)
    lax.fori_loop(NORM_A, NORM_B, norm_rows, 0)
    send(dn_piece(g, x, k), dn_piece(g, x, k), DNG, to_gr)
    lax.fori_loop(NORM_B, TOK // 16, norm_rows, 0)

    for u in range(2):
        for j, _ in sources:
            q, w = j // 2, j % 2
            start = ((a_me + 4 * q) * 4 + 2 * ok + w) * 64
            slot = up_buf.at[pl.ds(pl.multiple_of(start, 64), 64), pl.ds(u * HALF, HALF)]
            arrived(slot, UP1 + u * 4 + j)
            if w == 1:
                piece = up_piece(x, q, k, u)
                for d in range(3):
                    send(piece, piece, UPX + u * 6 + q * 3 + d, x_to[d])
                send(piece, piece, UPC + u * 8 + q * 4, to_core)

    def up_to_core(u):
        for d in (1, 2, 0):
            for q in range(2):
                piece = up_piece(x_from[d], q, k, u)
                arrived(piece, UPX + u * 6 + q * 3 + d)
                send(piece, piece, UPC + u * 8 + q * 4 + 1 + d, to_core)

    def hidden_half(u):
        for q in range(2):
            arrived(up_piece(x, q, ok, u), UPC + u * 8 + q * 4)
            for d in range(3):
                arrived(up_piece(x_from[d], q, ok, u), UPC + u * 8 + q * 4 + 1 + d)
        _, count, size = H_CHUNKS[u]
        units = pl.ds(u * HALF, HALF)
        for part in range(2):
            at = pl.ds(part * 256, 256)
            pre = jnp.dot(nrm[at, :], up_buf[:, units], preferred_element_type=F32)
            pre = jnp.maximum(pre, 0.0)
            h_buf[y, at, units] = (pre * pre).astype(BF16)
            for j in range(part * count // 2, (part + 1) * count // 2):
                piece = h_buf.at[y, pl.ds(j * size, size), units]
                for d in range(3):
                    send(piece, piece, HY + u * 6 + j * 3 + d, y_to[d])

    dt_over_core(0)
    up_to_core(0)
    arrived(dn_piece(og, x, k), DNG)
    dt_other = dn_buf[:, dn_cols(og, x, k)].astype(F32).T.astype(BF16)
    for h in range(2):
        dt_send[1, h] = dt_other[h * 64 : (h + 1) * 64]
    dt_over_y(1)

    hidden_half(0)

    dt_over_x(1)
    up_to_core(1)
    hidden_half(1)

    dn_over_x(1)

    dt_over_core(1)

    @pl.when(jnp.logical_not(owner))
    def _():
        for part in range(2):
            arrived(dt_piece(part, x), DTC + part * 4)
            for d in range(3):
                arrived(dt_piece(part, x_from[d]), DTC + part * 4 + 1 + d)

    def times_hidden(rows_at, size, at):
        total = jnp.zeros((size, TC), F32)
        for yy in range(4):
            total += lax.dot_general(
                dt_buf[yy, rows_at, :], h_buf[yy, at, :],
                (((1,), (1,)), ((), ())), preferred_element_type=F32,
            )
        return total

    def aligned(start, size):
        return pl.ds(pl.multiple_of(start, 64), size)

    def hidden_in(u, j):
        _, _, size = H_CHUNKS[u]
        for d in range(3):
            arrived(h_buf.at[y_from[d], pl.ds(j * size, size), pl.ds(u * HALF, HALF)], HY + u * 6 + j * 3 + d)

    for j in range(NT):
        at = pl.ds(j * TC, TC)
        if j % (NT // 2) == 0:
            hidden_in(0, j // (NT // 2))
        hidden_in(1, j)
        s1[j] = times_hidden(aligned((1 - b0) * 256, 256), 256, at).astype(BF16)
        send(s1.at[j], r1.at[j], RS + 3 * j, to_z1)
        k1[j] = times_hidden(aligned(b0 * 256, 256), 256, at)

    for j in range(NT):
        arrived(r1.at[j], RS + 3 * j)
        out, keep = aligned((1 - b1) * 128, 128), aligned(b1 * 128, 128)
        s2[j] = (k1[j, out, :] + r1[j, out, :].astype(F32)).astype(BF16)
        send(s2.at[j], r2.at[j], RS + 3 * j + 1, to_z2)
        k2[j] = k1[j, keep, :] + r1[j, keep, :].astype(F32)
    for j in range(NT):
        arrived(r2.at[j], RS + 3 * j + 1)
        out, keep = aligned((1 - b2) * 64, 64), aligned(b2 * 64, 64)
        s3[j] = (k2[j, out, :] + r2[j, out, :].astype(F32)).astype(BF16)
        send(s3.at[j], r3.at[j], RS + 3 * j + 2, to_z4)
        k3[j] = k2[j, keep, :] + r2[j, keep, :].astype(F32)

    dn_over_core(0)
    dn_over_core(1)

    for part in range(2):
        arrived(dn_piece(halves[part], x, ok), DNC + part * 4)
        for d in range(3):
            arrived(dn_piece(halves[part], x_from[d], ok), DNC + part * 4 + 1 + d)

    for j in range(NT):
        arrived(r3.at[j], RS + 3 * j + 2)
        mix_ref[:, j * TC : (j + 1) * TC] = (k3[j] + r3[j].astype(F32)).astype(BF16)

    for copy in sent:
        copy.wait_send()
    for part in range(2):
        for h in range(2):

            @pl.when(2 * k + h != y)
            def _():
                dt_to_y(part, h).wait_send()

        @pl.when(owner)
        def _():
            for copy in dt_from_x(part):
                copy.wait_send()
            for d in range(3):
                dt_to_core(part, d).wait_send()


def write_out(up_ref, dn_ref, mix_ref, up_hbm, dn_hbm, mix_hbm, lsem):
    copies = [
        pltpu.make_async_copy(src, dst, lsem.at[i])
        for i, (src, dst) in enumerate(((up_ref, up_hbm), (dn_ref, dn_hbm), (mix_ref, mix_hbm)))
    ]
    for copy in copies:
        copy.start()
    for copy in copies:
        copy.wait()


def per_device(tokens, norm_gain, up_weight, down_weight):
    hbm = pl.BlockSpec(memory_space=pltpu.HBM)
    vmem = pl.BlockSpec(memory_space=pltpu.VMEM)
    up_block, down_block, mixed = pl.pallas_call(
        kernel,
        out_shape=(
            jax.ShapeDtypeStruct((D, UNITS), BF16),
            jax.ShapeDtypeStruct((UNITS, D), BF16),
            jax.ShapeDtypeStruct((64, TOK), BF16),
        ),
        in_specs=[hbm] * 4,
        out_specs=(vmem,) * 3,
        scratch_shapes=[
            pltpu.VMEM((1, 64), F32),
            pltpu.VMEM((64, 512), F32),
            pltpu.VMEM((256, 128), F32),
            pltpu.VMEM((2, 64, 256), BF16),
            pltpu.VMEM((2, 2, 64, 256), BF16),
            pltpu.VMEM((4, 512, 256), BF16),
            pltpu.VMEM((TOK, D), BF16),
            pltpu.VMEM((4, TOK, UNITS), BF16),
            pltpu.VMEM((NT, 256, TC), BF16),
            pltpu.VMEM((NT, 256, TC), BF16),
            pltpu.VMEM((NT, 256, TC), F32),
            pltpu.VMEM((NT, 128, TC), BF16),
            pltpu.VMEM((NT, 128, TC), BF16),
            pltpu.VMEM((NT, 128, TC), F32),
            pltpu.VMEM((NT, 64, TC), BF16),
            pltpu.VMEM((NT, 64, TC), BF16),
            pltpu.VMEM((NT, 64, TC), F32),
            pltpu.SemaphoreType.DMA((N_MSG,)),
            pltpu.SemaphoreType.DMA((N_MSG,)),
            pltpu.SemaphoreType.DMA((4,)),
        ],
        compiler_params=pltpu.CompilerParams(
            collective_id=0, has_side_effects=True, vmem_limit_bytes=16 * 1024 * 1024
        ),
        name="handoff",
    )(*(
        pltpu.with_memory_space_constraint(a, pltpu.HBM)
        for a in (tokens, norm_gain.reshape(1, 64), up_weight, down_weight)
    ))
    results = (up_block, down_block, mixed)
    up_block, down_block, mixed = pl.pallas_call(
        write_out,
        out_shape=tuple(jax.ShapeDtypeStruct(a.shape, a.dtype) for a in results),
        in_specs=[vmem] * 3,
        out_specs=(hbm,) * 3,
        scratch_shapes=[pltpu.SemaphoreType.DMA((3,))],
        compiler_params=pltpu.CompilerParams(vmem_limit_bytes=8 * 1024 * 1024),
        name="write_out",
    )(*results)
    return up_block, down_block, mixed.T


def solution(mesh):
    in_specs = (P(("gr", "tp"), None), P("fs"), P("fs", ("gr", "tp")), P("fs", ("gr", "tp")))
    out_specs = (P(None, "fs"), P("fs", None), P(("gr", "tp"), "fs"))
    return jax.shard_map(
        per_device, mesh=mesh, in_specs=in_specs, out_specs=out_specs, check_vma=False
    )
```

```python
import jax
import jax.numpy as jnp
from jax import lax
from jax.experimental import pallas as pl
from jax.experimental.pallas import tpu as pltpu
from jax.sharding import PartitionSpec as P

MESH = pl.DeviceIdType.MESH
F32 = jnp.float32
BF16 = jnp.bfloat16

TOK = 512
D = 2048
UNITS = 256
HALF = 128
NT = 4
TC = TOK // NT
NORM_U, NORM_A, NORM_B = 18, 24, 32
WIDE = 256


def numbered(*sizes):
    firsts, at = [], 0
    for size in sizes:
        firsts.append(at)
        at += size
    return (*firsts, at)


UP1, UPF, UPX, UPC, DNG, DNX, DNC, DTY, DTX, DTC, HY, RS, N_MSG = numbered(
    8, 4, 12, 16, 1, 6, 8, 8, 6, 8, 12, 3 * NT
)


def kernel(
    tok_hbm, gain_hbm, upw_hbm, dnw_hbm,
    up_buf, dn_buf, mix_ref,
    gain_ref, upw_ref, dnw_ref,
    u_send, dt_send, dt_buf, nrm, h_buf,
    s1, r1, k1, s2, r2, k2, s3, r3, k3,
    ssem, rsem, lsem, far_sem,
):
    g = lax.axis_index("gr")
    f = lax.axis_index("fs")
    t = lax.axis_index("tp")
    zl, y = f // 4, f % 4
    x, k = t // 2, t % 2
    ok = 1 - k
    og = 1 - g

    def dev(gg, zz, yy, xx, kk):
        return (gg, zz * 4 + yy, xx * 2 + kk)

    def message(src, dst, i, to, j=None):
        return pltpu.make_async_remote_copy(
            src_ref=src, dst_ref=dst,
            send_sem=ssem.at[i], recv_sem=rsem.at[i if j is None else j],
            device_id=to, device_id_type=MESH,
        )

    sent = []

    def send(src, dst, i, to, j=None):
        copy = message(src, dst, i, to, j)
        copy.start()
        sent.append(copy)

    to_core = dev(g, zl, y, x, ok)

    def arrived(dst, i):
        message(dst, dst, 0, to_core, i).wait_recv()

    steps = (2, 1, 3)
    x_to = [dev(g, zl, y, (x + s) % 4, k) for s in steps]
    x_from = [(x + 4 - s) % 4 for s in steps]
    y_to = [dev(g, zl, (y + s) % 4, x, k) for s in steps]
    y_from = [(y + 4 - s) % 4 for s in steps]
    b0, b1, b2 = zl % 2, (zl // 2) % 2, zl // 4
    to_z1 = dev(g, zl + 1 - 2 * b0, y, x, k)
    to_z2 = dev(g, zl + 2 - 4 * b1, y, x, k)
    to_z4 = dev(g, zl + 4 - 8 * b2, y, x, k)
    to_gr = dev(og, zl, y, x, k)

    xs, ks, hs = zl % 4, y // 2, y % 2
    relayed = jnp.logical_and(g == 1, b2 == 0)
    relays = jnp.logical_and(g == 0, b2 == 0)

    def a_of(xx):
        return (xx - xs - hs - 2 * g * b2 + 8) % 4

    a_me = a_of(x)
    sources = [
        (q * 2 + w, dev(b2, a_me + 4 * q, 2 * ok + w, xs, ks)) for q in range(2) for w in range(2)
    ]

    barrier = pltpu.get_barrier_semaphore()

    def greet(who):
        pl.semaphore_signal(barrier, inc=1, device_id=who, device_id_type=MESH)

    @pl.when(jnp.logical_not(relayed))
    def _():
        for _, source in sources:
            greet(source)

    @pl.when(g == 0)
    def _():
        greet(to_gr)

    for who in (*x_to, *y_to, to_z1, to_z2, to_z4, to_core):
        greet(who)

    loads = [
        pltpu.make_async_copy(src, dst, lsem.at[i])
        for i, (src, dst) in enumerate(
            ((gain_hbm, gain_ref), (upw_hbm, upw_ref), (dnw_hbm, dnw_ref), (tok_hbm, nrm))
        )
    ]
    for load in loads:
        load.start()

    loads[0].wait()
    loads[1].wait()
    rows = lax.broadcasted_iota(jnp.int32, (64, 64), 0)
    cols = lax.broadcasted_iota(jnp.int32, (64, 64), 1)
    gain_wide = jnp.broadcast_to(gain_ref[...], (64, 64))
    gain = jnp.sum(jnp.where(rows == cols, gain_wide, 0.0), axis=1, keepdims=True)
    for h in range(2):
        u_send[h] = (gain * upw_ref[:, h * 256 : (h + 1) * 256]).astype(BF16)

    def dn_cols(gg, xx, kk):
        return pl.ds(pl.multiple_of((gg * 8 + xx * 2 + kk) * 128, 128), 128)

    def dn_piece(gg, xx, kk):
        return dn_buf.at[:, dn_cols(gg, xx, kk)]

    loads[2].wait()
    dn_mine = dnw_ref[...]
    dn_buf[:, dn_cols(g, x, k)] = dn_mine.astype(BF16)

    dt_mine = dn_mine.T.astype(BF16)
    for h in range(2):
        dt_send[0, h] = dt_mine[h * 64 : (h + 1) * 64]

    @pl.when(g == 0)
    def _():
        pl.semaphore_wait(barrier, 12)

    @pl.when(g == 1)
    def _():
        pl.semaphore_wait(barrier, 15)
        pl.semaphore_signal(far_sem, inc=1, device_id=to_gr, device_id_type=MESH)


    def up_piece(xx, q, kk, u):
        start = ((a_of(xx) + 4 * q) * 4 + 2 * (1 - kk)) * 64
        return up_buf.at[pl.ds(pl.multiple_of(start, 128), 128), pl.ds(u * HALF, HALF)]

    j_me = b2 * 2 + y % 2

    def up_message(u, gg, h):
        xx = (x + zl + h + 2 * gg) % 4
        to = (gg, (4 * g + x) * 4 + 2 * k + h, xx * 2 + (1 - y // 2))
        slot = up_buf.at[pl.ds(pl.multiple_of(f * 64, 64), 64), pl.ds(u * HALF, HALF)]
        src = u_send.at[h, :, pl.ds(u * HALF, HALF)]
        return message(src, slot, UP1 + u * 4 + gg * 2 + h, to, UP1 + u * 4 + j_me)

    def up_first(u):
        for h in range(2):
            up_message(u, 0, h).start()

        @pl.when(g == 1)
        def _():
            for h in range(2):
                up_message(u, 1, h).start()

    def up_relay(u, q):
        piece = up_piece(x, q, k, u)
        return message(piece, piece, UPF + u * 2 + q, to_gr)

    up_first(0)

    owner = ks == k
    halves = (g, og)

    def dt_rows(part, xx):
        return pl.ds(pl.multiple_of(((xx % 2) * 4 + (xx // 2) * 2 + halves[part]) * 64, 64), 64)

    def dt_piece(part, xx):
        return dt_buf.at[:, dt_rows(part, xx), :]

    def dt_to_y(part, h):
        return message(
            dt_send.at[part, h], dt_buf.at[y, dt_rows(part, x), :],
            DTY + part * 4 + h, dev(g, zl, 2 * k + h, x, k), DTY + part * 4 + y,
        )

    def dt_over_y(part):
        for h in range(2):

            @pl.when(2 * k + h != y)
            def _():
                dt_to_y(part, h).start()

            @pl.when(2 * k + h == y)
            def _():
                dt_buf[y, dt_rows(part, x), :] = dt_send[part, h]

    def dt_from_x(part):
        piece = dt_piece(part, x)
        return [message(piece, piece, DTX + part * 3 + d, x_to[d]) for d in range(3)] + [
            message(piece, piece, DTC + part * 4, to_core)
        ]

    def dt_over_x(part):
        @pl.when(owner)
        def _():
            for src in range(4):

                @pl.when(y != src)
                def _():
                    arrived(dt_buf.at[src, dt_rows(part, x), :], DTY + part * 4 + src)

            for copy in dt_from_x(part):
                copy.start()

    def dt_to_core(part, d):
        piece = dt_piece(part, x_from[d])
        return message(piece, piece, DTC + part * 4 + 1 + d, to_core)

    def dt_over_core(part):
        @pl.when(owner)
        def _():
            for d in (1, 2, 0):
                arrived(dt_piece(part, x_from[d]), DTX + part * 3 + d)
                dt_to_core(part, d).start()

    def dn_over_x(part):
        piece = dn_piece(halves[part], x, k)
        for d in range(3):
            send(piece, piece, DNX + part * 3 + d, x_to[d])
        send(piece, piece, DNC + part * 4, to_core)

    def dn_over_core(part):
        for d in (1, 2, 0):
            piece = dn_piece(halves[part], x_from[d], k)
            arrived(piece, DNX + part * 3 + d)
            send(piece, piece, DNC + part * 4 + 1 + d, to_core)

    dt_over_y(0)
    dn_over_x(0)

    loads[3].wait()

    def norm_rows(i, _):
        at = pl.ds(pl.multiple_of(i * 16, 16), 16)
        wide = nrm[at, :].astype(F32)
        scale = lax.rsqrt(jnp.mean(wide * wide, axis=-1, keepdims=True) + 1e-06)
        nrm[at, :] = (wide * scale).astype(BF16)
        return 0

    lax.fori_loop(0, NORM_U, norm_rows, 0)
    up_first(1)
    lax.fori_loop(NORM_U, NORM_A, norm_rows, 0)
    dt_over_x(0)
    lax.fori_loop(NORM_A, NORM_B, norm_rows, 0)
    lax.fori_loop(NORM_B, TOK // 16, norm_rows, 0)

    @pl.when(g == 0)
    def _():
        pl.semaphore_wait(far_sem, 1)

    def up_in(u):
        for q in range(2):

            @pl.when(relayed)
            def _():
                arrived(up_piece(x, q, k, u), UPF + u * 2 + q)

            @pl.when(jnp.logical_not(relayed))
            def _():
                for w in range(2):
                    start = ((a_me + 4 * q) * 4 + 2 * ok + w) * 64
                    slot = up_buf.at[pl.ds(pl.multiple_of(start, 64), 64), pl.ds(u * HALF, HALF)]
                    arrived(slot, UP1 + u * 4 + q * 2 + w)

            @pl.when(relays)
            def _():
                up_relay(u, q).start()

            piece = up_piece(x, q, k, u)
            for d in range(3):
                send(piece, piece, UPX + u * 6 + q * 3 + d, x_to[d])
            send(piece, piece, UPC + u * 8 + q * 4, to_core)

    send(dn_piece(g, x, k), dn_piece(g, x, k), DNG, to_gr)
    up_in(0)
    up_in(1)

    def up_to_core(u):
        for d in (1, 2, 0):
            for q in range(2):
                piece = up_piece(x_from[d], q, k, u)
                arrived(piece, UPX + u * 6 + q * 3 + d)
                send(piece, piece, UPC + u * 8 + q * 4 + 1 + d, to_core)

    def hidden_out(u, part):
        piece = h_buf.at[y, pl.ds(part * WIDE, WIDE), pl.ds(u * HALF, HALF)]
        for d in range(3):
            send(piece, piece, HY + u * 6 + part * 3 + d, y_to[d])

    def hidden_half(u):
        for q in range(2):
            arrived(up_piece(x, q, ok, u), UPC + u * 8 + q * 4)
            for d in range(3):
                arrived(up_piece(x_from[d], q, ok, u), UPC + u * 8 + q * 4 + 1 + d)
        units = pl.ds(u * HALF, HALF)
        for part in range(2):
            at = pl.ds(part * WIDE, WIDE)
            pre = jnp.dot(nrm[at, :], up_buf[:, units], preferred_element_type=F32)
            pre = jnp.maximum(pre, 0.0)
            h_buf[y, at, units] = (pre * pre).astype(BF16)
            if (u, part) != (0, 1):
                hidden_out(u, part)
            if (u, part) == (1, 0):
                hidden_out(0, 1)

    dt_over_core(0)
    up_to_core(0)
    arrived(dn_piece(og, x, k), DNG)
    dt_other = dn_buf[:, dn_cols(og, x, k)].astype(F32).T.astype(BF16)
    for h in range(2):
        dt_send[1, h] = dt_other[h * 64 : (h + 1) * 64]
    dt_over_y(1)

    hidden_half(0)

    dt_over_x(1)
    up_to_core(1)
    hidden_half(1)

    dn_over_x(1)

    dt_over_core(1)

    @pl.when(jnp.logical_not(owner))
    def _():
        for part in range(2):
            arrived(dt_piece(part, x), DTC + part * 4)
            for d in range(3):
                arrived(dt_piece(part, x_from[d]), DTC + part * 4 + 1 + d)

    def times_hidden(first, at):
        rows_at = pl.ds(pl.multiple_of(first, 256), 256)
        total = jnp.zeros((256, WIDE), F32)
        for yy in range(4):
            total += lax.dot_general(
                dt_buf[yy, rows_at, :], h_buf[yy, at, :],
                (((1,), (1,)), ((), ())), preferred_element_type=F32,
            )
        return total

    def aligned(start, size):
        return pl.ds(pl.multiple_of(start, 64), size)

    for part in range(2):
        at = pl.ds(part * WIDE, WIDE)
        for u in range(2):
            for d in range(3):
                piece = h_buf.at[y_from[d], at, pl.ds(u * HALF, HALF)]
                arrived(piece, HY + u * 6 + part * 3 + d)
        total = times_hidden((1 - b0) * 256, at).astype(BF16)
        for i in range(WIDE // TC):
            j = part * (WIDE // TC) + i
            s1[j] = total[:, i * TC : (i + 1) * TC]
            send(s1.at[j], r1.at[j], RS + 3 * j, to_z1)
    for part in range(2):
        total = times_hidden(b0 * 256, pl.ds(part * WIDE, WIDE))
        for i in range(WIDE // TC):
            k1[part * (WIDE // TC) + i] = total[:, i * TC : (i + 1) * TC]

    for j in range(NT):
        arrived(r1.at[j], RS + 3 * j)
        out, keep = aligned((1 - b1) * 128, 128), aligned(b1 * 128, 128)
        s2[j] = (k1[j, out, :] + r1[j, out, :].astype(F32)).astype(BF16)
        send(s2.at[j], r2.at[j], RS + 3 * j + 1, to_z2)
        k2[j] = k1[j, keep, :] + r1[j, keep, :].astype(F32)
    for j in range(NT):
        arrived(r2.at[j], RS + 3 * j + 1)
        out, keep = aligned((1 - b2) * 64, 64), aligned(b2 * 64, 64)
        s3[j] = (k2[j, out, :] + r2[j, out, :].astype(F32)).astype(BF16)
        send(s3.at[j], r3.at[j], RS + 3 * j + 2, to_z4)
        k3[j] = k2[j, keep, :] + r2[j, keep, :].astype(F32)

    dn_over_core(0)
    dn_over_core(1)

    for part in range(2):
        arrived(dn_piece(halves[part], x, ok), DNC + part * 4)
        for d in range(3):
            arrived(dn_piece(halves[part], x_from[d], ok), DNC + part * 4 + 1 + d)

    for j in range(NT):
        arrived(r3.at[j], RS + 3 * j + 2)
        mix_ref[:, j * TC : (j + 1) * TC] = (k3[j] + r3[j].astype(F32)).astype(BF16)

    for copy in sent:
        copy.wait_send()
    for u in range(2):
        for h in range(2):
            up_message(u, 0, h).wait_send()

        @pl.when(g == 1)
        def _():
            for h in range(2):
                up_message(u, 1, h).wait_send()

        @pl.when(relays)
        def _():
            for q in range(2):
                up_relay(u, q).wait_send()

    for part in range(2):
        for h in range(2):

            @pl.when(2 * k + h != y)
            def _():
                dt_to_y(part, h).wait_send()

        @pl.when(owner)
        def _():
            for copy in dt_from_x(part):
                copy.wait_send()
            for d in range(3):
                dt_to_core(part, d).wait_send()


def write_out(up_ref, dn_ref, mix_ref, up_hbm, dn_hbm, mix_hbm, lsem):
    copies = [
        pltpu.make_async_copy(src, dst, lsem.at[i])
        for i, (src, dst) in enumerate(((up_ref, up_hbm), (dn_ref, dn_hbm), (mix_ref, mix_hbm)))
    ]
    for copy in copies:
        copy.start()
    for copy in copies:
        copy.wait()


def per_device(tokens, norm_gain, up_weight, down_weight):
    hbm = pl.BlockSpec(memory_space=pltpu.HBM)
    vmem = pl.BlockSpec(memory_space=pltpu.VMEM)
    up_block, down_block, mixed = pl.pallas_call(
        kernel,
        out_shape=(
            jax.ShapeDtypeStruct((D, UNITS), BF16),
            jax.ShapeDtypeStruct((UNITS, D), BF16),
            jax.ShapeDtypeStruct((64, TOK), BF16),
        ),
        in_specs=[hbm] * 4,
        out_specs=(vmem,) * 3,
        scratch_shapes=[
            pltpu.VMEM((1, 64), F32),
            pltpu.VMEM((64, 512), F32),
            pltpu.VMEM((256, 128), F32),
            pltpu.VMEM((2, 64, 256), BF16),
            pltpu.VMEM((2, 2, 64, 256), BF16),
            pltpu.VMEM((4, 512, 256), BF16),
            pltpu.VMEM((TOK, D), BF16),
            pltpu.VMEM((4, TOK, UNITS), BF16),
            pltpu.VMEM((NT, 256, TC), BF16),
            pltpu.VMEM((NT, 256, TC), BF16),
            pltpu.VMEM((NT, 256, TC), F32),
            pltpu.VMEM((NT, 128, TC), BF16),
            pltpu.VMEM((NT, 128, TC), BF16),
            pltpu.VMEM((NT, 128, TC), F32),
            pltpu.VMEM((NT, 64, TC), BF16),
            pltpu.VMEM((NT, 64, TC), BF16),
            pltpu.VMEM((NT, 64, TC), F32),
            pltpu.SemaphoreType.DMA((N_MSG,)),
            pltpu.SemaphoreType.DMA((N_MSG,)),
            pltpu.SemaphoreType.DMA((4,)),
            pltpu.SemaphoreType.REGULAR,
        ],
        compiler_params=pltpu.CompilerParams(
            collective_id=0, has_side_effects=True, vmem_limit_bytes=16 * 1024 * 1024
        ),
        name="handoff",
    )(*(
        pltpu.with_memory_space_constraint(a, pltpu.HBM)
        for a in (tokens, norm_gain.reshape(1, 64), up_weight, down_weight)
    ))
    results = (up_block, down_block, mixed)
    up_block, down_block, mixed = pl.pallas_call(
        write_out,
        out_shape=tuple(jax.ShapeDtypeStruct(a.shape, a.dtype) for a in results),
        in_specs=[vmem] * 3,
        out_specs=(hbm,) * 3,
        scratch_shapes=[pltpu.SemaphoreType.DMA((3,))],
        compiler_params=pltpu.CompilerParams(vmem_limit_bytes=8 * 1024 * 1024),
        name="write_out",
    )(*results)
    return up_block, down_block, mixed.T


def solution(mesh):
    in_specs = (P(("gr", "tp"), None), P("fs"), P("fs", ("gr", "tp")), P("fs", ("gr", "tp")))
    out_specs = (P(None, "fs"), P("fs", None), P(("gr", "tp"), "fs"))
    return jax.shard_map(
        per_device, mesh=mesh, in_specs=in_specs, out_specs=out_specs, check_vma=False
    )
```

```python
import jax
import jax.numpy as jnp
from jax import lax
from jax.experimental import pallas as pl
from jax.experimental.pallas import tpu as pltpu
from jax.sharding import PartitionSpec as P

MESH = pl.DeviceIdType.MESH
F32 = jnp.float32
BF16 = jnp.bfloat16

TOK = 512
D = 2048
UNITS = 256
HALF = 128
NT = 4
TC = TOK // NT
NORM_U, NORM_A, NORM_B = 18, 24, 32


def numbered(*sizes):
    firsts, at = [], 0
    for size in sizes:
        firsts.append(at)
        at += size
    return (*firsts, at)


UP1, UPF, UPX, UPC, DNG, DNX, DNC, DTY, DTX, DTC, HY, RS, N_RECV = numbered(
    4, 4, 12, 2, 1, 2, 1, 2, 6, 1, NT, 3 * NT
)
S_W, S_L, S_G, S_R, S_Y, S_X, N_SEND = numbered(1, 1, 1, 1, 1, 1)
KIB = 1024


def kernel(
    tok_hbm, gain_hbm, upw_hbm, dnw_hbm,
    up_buf, dn_buf, mix_ref,
    gain_ref, upw_ref, dnw_ref,
    u_send, dt_send, dt_buf, nrm, h_buf,
    s1, r1, k1, s2, r2, k2, s3, r3, k3,
    ssem, rsem, lsem, far_sem,
):
    g = lax.axis_index("gr")
    f = lax.axis_index("fs")
    t = lax.axis_index("tp")
    zl, y = f // 4, f % 4
    x, k = t // 2, t % 2
    ok = 1 - k
    og = 1 - g

    def dev(gg, zz, yy, xx, kk):
        return (gg, zz * 4 + yy, xx * 2 + kk)

    def message(src, dst, i, to, group):
        return pltpu.make_async_remote_copy(
            src_ref=src, dst_ref=dst, send_sem=ssem.at[group], recv_sem=rsem.at[i],
            device_id=to, device_id_type=MESH,
        )

    def send(src, dst, i, to, group=S_W):
        message(src, dst, i, to, group).start()

    to_core = dev(g, zl, y, x, ok)

    def arrived(landed, i):
        message(landed, landed, i, to_core, S_W).wait_recv()

    def all_left(group, size):
        rows = nrm.at[pl.ds(0, size // (2 * D)), :]
        message(rows, rows, 0, to_core, group).wait_send()

    steps = (2, 1, 3)
    x_to = [dev(g, zl, y, (x + s) % 4, k) for s in steps]
    x_from = [(x + 4 - s) % 4 for s in steps]
    y_to = [dev(g, zl, (y + s) % 4, x, k) for s in steps]
    y_from = [(y + 4 - s) % 4 for s in steps]
    b0, b1, b2 = zl % 2, (zl // 2) % 2, zl // 4
    to_z1 = dev(g, zl + 1 - 2 * b0, y, x, k)
    to_z2 = dev(g, zl + 2 - 4 * b1, y, x, k)
    to_z4 = dev(g, zl + 4 - 8 * b2, y, x, k)
    to_gr = dev(og, zl, y, x, k)

    xs, ks, hs = zl % 4, y // 2, y % 2
    relayed = jnp.logical_and(g == 1, b2 == 0)
    relays = jnp.logical_and(g == 0, b2 == 0)

    def a_of(xx):
        return (xx - xs - hs - 2 * g * b2 + 8) % 4

    a_me = a_of(x)
    sources = [
        (q * 2 + w, dev(b2, a_me + 4 * q, 2 * ok + w, xs, ks)) for q in range(2) for w in range(2)
    ]

    barrier = pltpu.get_barrier_semaphore()

    def greet(who):
        pl.semaphore_signal(barrier, inc=1, device_id=who, device_id_type=MESH)

    @pl.when(jnp.logical_not(relayed))
    def _():
        for _, source in sources:
            greet(source)

    @pl.when(g == 0)
    def _():
        greet(to_gr)

    for who in (*x_to, *y_to, to_z1, to_z2, to_z4, to_core):
        greet(who)

    loads = [
        pltpu.make_async_copy(src, dst, lsem.at[i])
        for i, (src, dst) in enumerate(
            ((gain_hbm, gain_ref), (upw_hbm, upw_ref), (dnw_hbm, dnw_ref), (tok_hbm, nrm))
        )
    ]
    for load in loads:
        load.start()

    loads[0].wait()
    loads[1].wait()
    rows = lax.broadcasted_iota(jnp.int32, (64, 64), 0)
    cols = lax.broadcasted_iota(jnp.int32, (64, 64), 1)
    gain_wide = jnp.broadcast_to(gain_ref[...], (64, 64))
    gain = jnp.sum(jnp.where(rows == cols, gain_wide, 0.0), axis=1, keepdims=True)
    for h in range(2):
        u_send[h] = (gain * upw_ref[:, h * 256 : (h + 1) * 256]).astype(BF16)

    def dn_cols(gg, xx, kk):
        return pl.ds(pl.multiple_of((gg * 8 + xx * 2 + kk) * 128, 128), 128)

    def dn_piece(gg, xx, kk):
        return dn_buf.at[:, dn_cols(gg, xx, kk)]

    loads[2].wait()
    dn_mine = dnw_ref[...]
    dn_buf[:, dn_cols(g, x, k)] = dn_mine.astype(BF16)

    dt_mine = dn_mine.T.astype(BF16)
    for h in range(2):
        dt_send[0, h] = dt_mine[h * 64 : (h + 1) * 64]

    @pl.when(g == 0)
    def _():
        pl.semaphore_wait(barrier, 12)

    @pl.when(g == 1)
    def _():
        pl.semaphore_wait(barrier, 15)
        pl.semaphore_signal(far_sem, inc=1, device_id=to_gr, device_id_type=MESH)


    def up_piece(xx, q, kk, u):
        start = ((a_of(xx) + 4 * q) * 4 + 2 * (1 - kk)) * 64
        return up_buf.at[pl.ds(pl.multiple_of(start, 128), 128), pl.ds(u * HALF, HALF)]

    def up_message(u, gg, h):
        xx = (x + zl + h + 2 * gg) % 4
        to = (gg, (4 * g + x) * 4 + 2 * k + h, xx * 2 + (1 - y // 2))
        slot = up_buf.at[pl.ds(pl.multiple_of(f * 64, 64), 64), pl.ds(u * HALF, HALF)]
        src = u_send.at[h, :, pl.ds(u * HALF, HALF)]
        return message(src, slot, UP1 + u * 2 + b2, to, (S_W, S_G)[gg])

    def up_first(u):
        for h in range(2):
            up_message(u, 0, h).start()

        @pl.when(g == 1)
        def _():
            for h in range(2):
                up_message(u, 1, h).start()

    def up_relay(u, q):
        piece = up_piece(x, q, k, u)
        return message(piece, piece, UPF + u * 2 + q, to_gr, S_R)

    up_first(0)

    owner = ks == k
    halves = (g, og)

    def dt_rows(part, xx):
        return pl.ds(pl.multiple_of(((xx % 2) * 4 + (xx // 2) * 2 + halves[part]) * 64, 64), 64)

    def dt_piece(part, xx):
        return dt_buf.at[:, dt_rows(part, xx), :]

    def dt_to_y(part, h):
        return message(
            dt_send.at[part, h], dt_buf.at[y, dt_rows(part, x), :],
            DTY + part, dev(g, zl, 2 * k + h, x, k), S_Y,
        )

    def dt_over_y(part):
        for h in range(2):

            @pl.when(2 * k + h != y)
            def _():
                dt_to_y(part, h).start()

            @pl.when(2 * k + h == y)
            def _():
                dt_buf[y, dt_rows(part, x), :] = dt_send[part, h]

    def dt_from_x(part):
        piece = dt_piece(part, x)
        return [message(piece, piece, DTX + part * 3 + d, x_to[d], S_X) for d in range(3)] + [
            message(piece, piece, DTC, to_core, S_X)
        ]

    def dt_over_x(part):
        @pl.when(owner)
        def _():
            arrived(dt_buf.at[pl.ds(0, 3), dt_rows(part, x), :], DTY + part)
            for copy in dt_from_x(part):
                copy.start()

    def dt_to_core(part, d):
        piece = dt_piece(part, x_from[d])
        return message(piece, piece, DTC, to_core, S_X)

    def dt_over_core(part):
        @pl.when(owner)
        def _():
            for d in (1, 2, 0):
                arrived(dt_piece(part, x_from[d]), DTX + part * 3 + d)
                dt_to_core(part, d).start()

    def dn_over_x(part):
        piece = dn_piece(halves[part], x, k)
        for d in range(3):
            send(piece, piece, DNX + part, x_to[d])
        send(piece, piece, DNC, to_core)

    def dn_over_core(part):
        arrived(dn_buf.at[:, pl.ds(0, 3 * 128)], DNX + part)
        for d in range(3):
            piece = dn_piece(halves[part], x_from[d], k)
            send(piece, piece, DNC, to_core)

    dt_over_y(0)
    dn_over_x(0)

    loads[3].wait()

    def norm_rows(i, _):
        at = pl.ds(pl.multiple_of(i * 16, 16), 16)
        wide = nrm[at, :].astype(F32)
        scale = lax.rsqrt(jnp.mean(wide * wide, axis=-1, keepdims=True) + 1e-06)
        nrm[at, :] = (wide * scale).astype(BF16)
        return 0

    lax.fori_loop(0, NORM_U, norm_rows, 0)
    up_first(1)
    lax.fori_loop(NORM_U, NORM_A, norm_rows, 0)
    dt_over_x(0)
    lax.fori_loop(NORM_A, NORM_B, norm_rows, 0)
    lax.fori_loop(NORM_B, TOK // 16, norm_rows, 0)

    @pl.when(g == 0)
    def _():
        pl.semaphore_wait(far_sem, 1)

    def up_in(u):
        for q in range(2):

            @pl.when(relayed)
            def _():
                arrived(up_piece(x, q, k, u), UPF + u * 2 + q)

            @pl.when(jnp.logical_not(relayed))
            def _():
                arrived(up_piece(x, q, k, u), UP1 + u * 2 + q)

            @pl.when(relays)
            def _():
                up_relay(u, q).start()

            piece = up_piece(x, q, k, u)
            for d in range(3):
                send(piece, piece, UPX + u * 6 + q * 3 + d, x_to[d])
            send(piece, piece, UPC + u, to_core)

    send(dn_piece(g, x, k), dn_piece(g, x, k), DNG, to_gr)
    up_in(0)
    up_in(1)

    def up_to_core(u):
        for d in (1, 2, 0):
            for q in range(2):
                piece = up_piece(x_from[d], q, k, u)
                arrived(piece, UPX + u * 6 + q * 3 + d)
                send(piece, piece, UPC + u, to_core)

    def hidden_out(u, j):
        piece = h_buf.at[y, pl.ds(j * TC, TC), pl.ds(u * HALF, HALF)]
        for d in range(3):
            send(piece, piece, HY + j, y_to[d], S_L)

    def hidden_half(u, order):
        arrived(up_buf.at[pl.ds(0, D // 2), pl.ds(u * HALF, HALF)], UPC + u)
        units = pl.ds(u * HALF, HALF)
        for part in range(2):
            at = pl.ds(part * TOK // 2, TOK // 2)
            pre = jnp.dot(nrm[at, :], up_buf[:, units], preferred_element_type=F32)
            pre = jnp.maximum(pre, 0.0)
            h_buf[y, at, units] = (pre * pre).astype(BF16)
            for uu, j in order[part]:
                hidden_out(uu, j)

    dt_over_core(0)
    up_to_core(0)
    arrived(dn_piece(og, x, k), DNG)
    dt_other = dn_buf[:, dn_cols(og, x, k)].astype(F32).T.astype(BF16)
    for h in range(2):
        dt_send[1, h] = dt_other[h * 64 : (h + 1) * 64]
    dt_over_y(1)

    hidden_half(0, (((0, 0), (0, 1)), ((0, 2),)))

    dt_over_x(1)
    up_to_core(1)
    hidden_half(1, (((1, 0), (1, 1)), ((1, 2), (0, 3), (1, 3))))

    dn_over_x(1)

    dt_over_core(1)

    @pl.when(jnp.logical_not(owner))
    def _():
        arrived(dt_buf, DTC)

    def times_hidden(first, j):
        rows_at = pl.ds(pl.multiple_of(first, 256), 256)
        total = jnp.zeros((256, TC), F32)
        for yy in range(4):
            total += lax.dot_general(
                dt_buf[yy, rows_at, :], h_buf[yy, pl.ds(j * TC, TC), :],
                (((1,), (1,)), ((), ())), preferred_element_type=F32,
            )
        return total

    def aligned(start, size):
        return pl.ds(pl.multiple_of(start, 64), size)

    def second_matmul(j):
        arrived(h_buf.at[pl.ds(0, 3), pl.ds(0, TC), :], HY + j)
        s1[j] = times_hidden((1 - b0) * 256, j).astype(BF16)
        send(s1.at[j], r1.at[j], RS + 3 * j, to_z1, S_L)
        k1[j] = times_hidden(b0 * 256, j)

    def halve(j):
        arrived(r1.at[j], RS + 3 * j)
        out, keep = aligned((1 - b1) * 128, 128), aligned(b1 * 128, 128)
        s2[j] = (k1[j, out, :] + r1[j, out, :].astype(F32)).astype(BF16)
        send(s2.at[j], r2.at[j], RS + 3 * j + 1, to_z2, S_L)
        k2[j] = k1[j, keep, :] + r1[j, keep, :].astype(F32)

    for j in range(NT):
        second_matmul(j)
        if j >= 2:
            halve(j - 2)
    halve(NT - 2)
    halve(NT - 1)
    for j in range(NT):
        arrived(r2.at[j], RS + 3 * j + 1)
        out, keep = aligned((1 - b2) * 64, 64), aligned(b2 * 64, 64)
        s3[j] = (k2[j, out, :] + r2[j, out, :].astype(F32)).astype(BF16)
        send(s3.at[j], r3.at[j], RS + 3 * j + 2, to_z4, S_L)
        k3[j] = k2[j, keep, :] + r2[j, keep, :].astype(F32)

    dn_over_core(0)
    dn_over_core(1)

    arrived(dn_buf.at[:, pl.ds(0, D // 2)], DNC)

    for j in range(NT):
        arrived(r3.at[j], RS + 3 * j + 2)
        mix_ref[:, j * TC : (j + 1) * TC] = (k3[j] + r3[j].astype(F32)).astype(BF16)

    all_left(S_W, (64 + 384 + 512 + 64 + 384 + 512) * KIB)
    all_left(S_L, (768 + 256 + 128 + 64) * KIB)

    @pl.when(g == 1)
    def _():
        all_left(S_G, 64 * KIB)

    @pl.when(relays)
    def _():
        all_left(S_R, 128 * KIB)

    @pl.when(owner)
    def _():
        all_left(S_Y, 64 * KIB)
        all_left(S_X, 2 * 7 * 128 * KIB)

    @pl.when(jnp.logical_not(owner))
    def _():
        all_left(S_Y, 128 * KIB)


def write_out(up_ref, dn_ref, mix_ref, up_hbm, dn_hbm, mix_hbm, lsem):
    copies = [
        pltpu.make_async_copy(src, dst, lsem.at[i])
        for i, (src, dst) in enumerate(((up_ref, up_hbm), (dn_ref, dn_hbm), (mix_ref, mix_hbm)))
    ]
    for copy in copies:
        copy.start()
    for copy in copies:
        copy.wait()


def per_device(tokens, norm_gain, up_weight, down_weight):
    hbm = pl.BlockSpec(memory_space=pltpu.HBM)
    vmem = pl.BlockSpec(memory_space=pltpu.VMEM)
    up_block, down_block, mixed = pl.pallas_call(
        kernel,
        out_shape=(
            jax.ShapeDtypeStruct((D, UNITS), BF16),
            jax.ShapeDtypeStruct((UNITS, D), BF16),
            jax.ShapeDtypeStruct((64, TOK), BF16),
        ),
        in_specs=[hbm] * 4,
        out_specs=(vmem,) * 3,
        scratch_shapes=[
            pltpu.VMEM((1, 64), F32),
            pltpu.VMEM((64, 512), F32),
            pltpu.VMEM((256, 128), F32),
            pltpu.VMEM((2, 64, 256), BF16),
            pltpu.VMEM((2, 2, 64, 256), BF16),
            pltpu.VMEM((4, 512, 256), BF16),
            pltpu.VMEM((TOK, D), BF16),
            pltpu.VMEM((4, TOK, UNITS), BF16),
            pltpu.VMEM((NT, 256, TC), BF16),
            pltpu.VMEM((NT, 256, TC), BF16),
            pltpu.VMEM((NT, 256, TC), F32),
            pltpu.VMEM((NT, 128, TC), BF16),
            pltpu.VMEM((NT, 128, TC), BF16),
            pltpu.VMEM((NT, 128, TC), F32),
            pltpu.VMEM((NT, 64, TC), BF16),
            pltpu.VMEM((NT, 64, TC), BF16),
            pltpu.VMEM((NT, 64, TC), F32),
            pltpu.SemaphoreType.DMA((N_SEND,)),
            pltpu.SemaphoreType.DMA((N_RECV,)),
            pltpu.SemaphoreType.DMA((4,)),
            pltpu.SemaphoreType.REGULAR,
        ],
        compiler_params=pltpu.CompilerParams(
            collective_id=0, has_side_effects=True, vmem_limit_bytes=16 * 1024 * 1024
        ),
        name="handoff",
    )(*(
        pltpu.with_memory_space_constraint(a, pltpu.HBM)
        for a in (tokens, norm_gain.reshape(1, 64), up_weight, down_weight)
    ))
    results = (up_block, down_block, mixed)
    up_block, down_block, mixed = pl.pallas_call(
        write_out,
        out_shape=tuple(jax.ShapeDtypeStruct(a.shape, a.dtype) for a in results),
        in_specs=[vmem] * 3,
        out_specs=(hbm,) * 3,
        scratch_shapes=[pltpu.SemaphoreType.DMA((3,))],
        compiler_params=pltpu.CompilerParams(vmem_limit_bytes=8 * 1024 * 1024),
        name="write_out",
    )(*results)
    return up_block, down_block, mixed.T


def solution(mesh):
    in_specs = (P(("gr", "tp"), None), P("fs"), P("fs", ("gr", "tp")), P("fs", ("gr", "tp")))
    out_specs = (P(None, "fs"), P("fs", None), P(("gr", "tp"), "fs"))
    return jax.shard_map(
        per_device, mesh=mesh, in_specs=in_specs, out_specs=out_specs, check_vma=False
    )
```

```python
import jax
import jax.numpy as jnp
from jax import lax
from jax.experimental import pallas as pl
from jax.experimental.pallas import tpu as pltpu
from jax.sharding import PartitionSpec as P

MESH = pl.DeviceIdType.MESH
F32 = jnp.float32
BF16 = jnp.bfloat16

TOK = 512
D = 2048
UNITS = 256
HALF = 128
NT = 4
TC = TOK // NT
STEPS = (3, 3, 2, 2)
NORM_U, NORM_A, NORM_B = 18, 24, 32


def numbered(*sizes):
    firsts, at = [], 0
    for size in sizes:
        firsts.append(at)
        at += size
    return (*firsts, at)


UP1, UPF, UPX, UPC, DNG, DNX, DNC, DTY, DTX, DTC, HY, RS, N_RECV = numbered(
    4, 4, 12, 2, 1, 2, 1, 2, 6, 1, NT, 3 * NT
)
S_W, S_L, S_G, S_R, S_Y, S_X, N_SEND = numbered(1, 1, 1, 1, 1, 1)
KIB = 1024
MATES = tuple(range(1, 8)) if 1 in STEPS else (1, 2, 4, 6) if 2 in STEPS else (1, 2, 4)


def kernel(
    tok_hbm, gain_hbm, upw_hbm, dnw_hbm,
    up_buf, dn_buf, mix_ref,
    gain_ref, upw_ref, dnw_ref,
    u_send, dt_send, dt_buf, nrm, h_buf,
    s1, r1, k1, s2, r2, k2, s3, r3, k3,
    sm, rm, sd, rd, kd,
    ssem, rsem, lsem, far_sem,
):
    g = lax.axis_index("gr")
    f = lax.axis_index("fs")
    t = lax.axis_index("tp")
    zl, y = f // 4, f % 4
    x, k = t // 2, t % 2
    ok = 1 - k
    og = 1 - g

    def dev(gg, zz, yy, xx, kk):
        return (gg, zz * 4 + yy, xx * 2 + kk)

    def message(src, dst, i, to, group):
        return pltpu.make_async_remote_copy(
            src_ref=src, dst_ref=dst, send_sem=ssem.at[group], recv_sem=rsem.at[i],
            device_id=to, device_id_type=MESH,
        )

    def send(src, dst, i, to, group=S_W):
        message(src, dst, i, to, group).start()

    to_core = dev(g, zl, y, x, ok)

    def arrived(landed, i):
        message(landed, landed, i, to_core, S_W).wait_recv()

    def all_left(group, size):
        rows = nrm.at[pl.ds(0, size // (2 * D)), :]
        message(rows, rows, 0, to_core, group).wait_send()

    steps = (2, 1, 3)
    x_to = [dev(g, zl, y, (x + s) % 4, k) for s in steps]
    x_from = [(x + 4 - s) % 4 for s in steps]
    y_to = [dev(g, zl, (y + s) % 4, x, k) for s in steps]
    y_from = [(y + 4 - s) % 4 for s in steps]
    b0, b1, b2 = zl % 2, (zl // 2) % 2, zl // 4
    to_z1 = dev(g, zl + 1 - 2 * b0, y, x, k)
    to_z2 = dev(g, zl + 2 - 4 * b1, y, x, k)
    to_z4 = dev(g, zl + 4 - 8 * b2, y, x, k)
    to_gr = dev(og, zl, y, x, k)

    place = b0 * 4 + b1 * 2 + b2

    def z_mate(m):
        flip = [abs(b - (m >> i) % 2) for i, b in enumerate((b0, b1, b2))]
        return dev(g, flip[0] + 2 * flip[1] + 4 * flip[2], y, x, k), flip[0] * 4 + flip[1] * 2 + flip[2]


    xs, ks, hs = zl % 4, y // 2, y % 2
    relayed = jnp.logical_and(g == 1, b2 == 0)
    relays = jnp.logical_and(g == 0, b2 == 0)

    def a_of(xx):
        return (xx - xs - hs - 2 * g * b2 + 8) % 4

    a_me = a_of(x)
    sources = [
        (q * 2 + w, dev(b2, a_me + 4 * q, 2 * ok + w, xs, ks)) for q in range(2) for w in range(2)
    ]

    barrier = pltpu.get_barrier_semaphore()

    def greet(who):
        pl.semaphore_signal(barrier, inc=1, device_id=who, device_id_type=MESH)

    @pl.when(jnp.logical_not(relayed))
    def _():
        for _, source in sources:
            greet(source)

    @pl.when(g == 0)
    def _():
        greet(to_gr)

    for who in (*x_to, *y_to, to_core, *(z_mate(m)[0] for m in MATES)):
        greet(who)

    loads = [
        pltpu.make_async_copy(src, dst, lsem.at[i])
        for i, (src, dst) in enumerate(
            ((gain_hbm, gain_ref), (upw_hbm, upw_ref), (dnw_hbm, dnw_ref), (tok_hbm, nrm))
        )
    ]
    for load in loads:
        load.start()

    loads[0].wait()
    loads[1].wait()
    rows = lax.broadcasted_iota(jnp.int32, (64, 64), 0)
    cols = lax.broadcasted_iota(jnp.int32, (64, 64), 1)
    gain_wide = jnp.broadcast_to(gain_ref[...], (64, 64))
    gain = jnp.sum(jnp.where(rows == cols, gain_wide, 0.0), axis=1, keepdims=True)
    for h in range(2):
        u_send[h] = (gain * upw_ref[:, h * 256 : (h + 1) * 256]).astype(BF16)

    def dn_cols(gg, xx, kk):
        return pl.ds(pl.multiple_of((gg * 8 + xx * 2 + kk) * 128, 128), 128)

    def dn_piece(gg, xx, kk):
        return dn_buf.at[:, dn_cols(gg, xx, kk)]

    loads[2].wait()
    dn_mine = dnw_ref[...]
    dn_buf[:, dn_cols(g, x, k)] = dn_mine.astype(BF16)

    dt_mine = dn_mine.T.astype(BF16)
    for h in range(2):
        dt_send[0, h] = dt_mine[h * 64 : (h + 1) * 64]

    @pl.when(g == 0)
    def _():
        pl.semaphore_wait(barrier, 9 + len(MATES))

    @pl.when(g == 1)
    def _():
        pl.semaphore_wait(barrier, 12 + len(MATES))
        pl.semaphore_signal(far_sem, inc=1, device_id=to_gr, device_id_type=MESH)


    def up_piece(xx, q, kk, u):
        start = ((a_of(xx) + 4 * q) * 4 + 2 * (1 - kk)) * 64
        return up_buf.at[pl.ds(pl.multiple_of(start, 128), 128), pl.ds(u * HALF, HALF)]

    def up_message(u, gg, h):
        xx = (x + zl + h + 2 * gg) % 4
        to = (gg, (4 * g + x) * 4 + 2 * k + h, xx * 2 + (1 - y // 2))
        slot = up_buf.at[pl.ds(pl.multiple_of(f * 64, 64), 64), pl.ds(u * HALF, HALF)]
        src = u_send.at[h, :, pl.ds(u * HALF, HALF)]
        return message(src, slot, UP1 + u * 2 + b2, to, (S_W, S_G)[gg])

    def up_first(u):
        for h in range(2):
            up_message(u, 0, h).start()

        @pl.when(g == 1)
        def _():
            for h in range(2):
                up_message(u, 1, h).start()

    def up_relay(u, q):
        piece = up_piece(x, q, k, u)
        return message(piece, piece, UPF + u * 2 + q, to_gr, S_R)

    up_first(0)

    owner = ks == k
    halves = (g, og)

    def dt_rows(part, xx):
        return pl.ds(pl.multiple_of(((xx % 2) * 4 + (xx // 2) * 2 + halves[part]) * 64, 64), 64)

    def dt_piece(part, xx):
        return dt_buf.at[:, dt_rows(part, xx), :]

    def dt_to_y(part, h):
        return message(
            dt_send.at[part, h], dt_buf.at[y, dt_rows(part, x), :],
            DTY + part, dev(g, zl, 2 * k + h, x, k), S_Y,
        )

    def dt_over_y(part):
        for h in range(2):

            @pl.when(2 * k + h != y)
            def _():
                dt_to_y(part, h).start()

            @pl.when(2 * k + h == y)
            def _():
                dt_buf[y, dt_rows(part, x), :] = dt_send[part, h]

    def dt_from_x(part):
        piece = dt_piece(part, x)
        return [message(piece, piece, DTX + part * 3 + d, x_to[d], S_X) for d in range(3)] + [
            message(piece, piece, DTC, to_core, S_X)
        ]

    def dt_over_x(part):
        @pl.when(owner)
        def _():
            arrived(dt_buf.at[pl.ds(0, 3), dt_rows(part, x), :], DTY + part)
            for copy in dt_from_x(part):
                copy.start()

    def dt_to_core(part, d):
        piece = dt_piece(part, x_from[d])
        return message(piece, piece, DTC, to_core, S_X)

    def dt_over_core(part):
        @pl.when(owner)
        def _():
            for d in (1, 2, 0):
                arrived(dt_piece(part, x_from[d]), DTX + part * 3 + d)
                dt_to_core(part, d).start()

    def dn_over_x(part):
        piece = dn_piece(halves[part], x, k)
        for d in range(3):
            send(piece, piece, DNX + part, x_to[d])
        send(piece, piece, DNC, to_core)

    def dn_over_core(part):
        arrived(dn_buf.at[:, pl.ds(0, 3 * 128)], DNX + part)
        for d in range(3):
            piece = dn_piece(halves[part], x_from[d], k)
            send(piece, piece, DNC, to_core)

    dt_over_y(0)
    dn_over_x(0)

    loads[3].wait()

    def norm_rows(i, _):
        at = pl.ds(pl.multiple_of(i * 16, 16), 16)
        wide = nrm[at, :].astype(F32)
        scale = lax.rsqrt(jnp.mean(wide * wide, axis=-1, keepdims=True) + 1e-06)
        nrm[at, :] = (wide * scale).astype(BF16)
        return 0

    lax.fori_loop(0, NORM_U, norm_rows, 0)
    up_first(1)
    lax.fori_loop(NORM_U, NORM_A, norm_rows, 0)
    dt_over_x(0)
    lax.fori_loop(NORM_A, NORM_B, norm_rows, 0)
    lax.fori_loop(NORM_B, TOK // 16, norm_rows, 0)

    @pl.when(g == 0)
    def _():
        pl.semaphore_wait(far_sem, 1)

    def up_in(u):
        for q in range(2):

            @pl.when(relayed)
            def _():
                arrived(up_piece(x, q, k, u), UPF + u * 2 + q)

            @pl.when(jnp.logical_not(relayed))
            def _():
                arrived(up_piece(x, q, k, u), UP1 + u * 2 + q)

            @pl.when(relays)
            def _():
                up_relay(u, q).start()

            piece = up_piece(x, q, k, u)
            for d in range(3):
                send(piece, piece, UPX + u * 6 + q * 3 + d, x_to[d])
            send(piece, piece, UPC + u, to_core)

    send(dn_piece(g, x, k), dn_piece(g, x, k), DNG, to_gr)
    up_in(0)
    up_in(1)

    def up_to_core(u):
        for d in (1, 2, 0):
            for q in range(2):
                piece = up_piece(x_from[d], q, k, u)
                arrived(piece, UPX + u * 6 + q * 3 + d)
                send(piece, piece, UPC + u, to_core)

    def hidden_out(u, j):
        piece = h_buf.at[y, pl.ds(j * TC, TC), pl.ds(u * HALF, HALF)]
        for d in range(3):
            send(piece, piece, HY + j, y_to[d], S_L)

    def hidden_half(u, order):
        arrived(up_buf.at[pl.ds(0, D // 2), pl.ds(u * HALF, HALF)], UPC + u)
        units = pl.ds(u * HALF, HALF)
        for part in range(2):
            at = pl.ds(part * TOK // 2, TOK // 2)
            pre = jnp.dot(nrm[at, :], up_buf[:, units], preferred_element_type=F32)
            pre = jnp.maximum(pre, 0.0)
            h_buf[y, at, units] = (pre * pre).astype(BF16)
            for uu, j in order[part]:
                hidden_out(uu, j)

    dt_over_core(0)
    up_to_core(0)
    arrived(dn_piece(og, x, k), DNG)
    dt_other = dn_buf[:, dn_cols(og, x, k)].astype(F32).T.astype(BF16)
    for h in range(2):
        dt_send[1, h] = dt_other[h * 64 : (h + 1) * 64]
    dt_over_y(1)

    hidden_half(0, (((0, 0), (0, 1)), ((0, 2),)))

    dt_over_x(1)
    up_to_core(1)
    hidden_half(1, (((1, 0), (1, 1)), ((1, 2), (0, 3), (1, 3))))

    dn_over_x(1)

    dt_over_core(1)

    @pl.when(jnp.logical_not(owner))
    def _():
        arrived(dt_buf, DTC)

    def times_hidden(first, j):
        rows_at = pl.ds(pl.multiple_of(first, 256), 256)
        total = jnp.zeros((256, TC), F32)
        for yy in range(4):
            total += lax.dot_general(
                dt_buf[yy, rows_at, :], h_buf[yy, pl.ds(j * TC, TC), :],
                (((1,), (1,)), ((), ())), preferred_element_type=F32,
            )
        return total

    def aligned(start, size):
        return pl.ds(pl.multiple_of(start, 64), size)

    def second_matmul(j):
        arrived(h_buf.at[pl.ds(0, 3), pl.ds(0, TC), :], HY + j)
        s1[j] = times_hidden((1 - b0) * 256, j).astype(BF16)
        send(s1.at[j], r1.at[j], RS + 3 * j, to_z1, S_L)
        k1[j] = times_hidden(b0 * 256, j)

    def halve(j):
        arrived(r1.at[j], RS + 3 * j)
        out, keep = aligned((1 - b1) * 128, 128), aligned(b1 * 128, 128)
        s2[j] = (k1[j, out, :] + r1[j, out, :].astype(F32)).astype(BF16)
        send(s2.at[j], r2.at[j], RS + 3 * j + 1, to_z2, S_L)
        k2[j] = k1[j, keep, :] + r1[j, keep, :].astype(F32)

    def halve_and_send(j):
        arrived(r1.at[j], RS + 3 * j)
        half_place = b1 * 2 + b2
        for m in (6, 4, 2):
            to, at_place = z_mate(m)
            at = at_place % 4
            rows_at = aligned(at * 64, 64)
            sm[j, at] = (k1[j, rows_at, :] + r1[j, rows_at, :].astype(F32)).astype(BF16)
            send(sm.at[j, at], rm.at[j, half_place], RS + 3 * j + 1, to, S_L)
        keep = aligned(half_place * 64, 64)
        k3[j] = k1[j, keep, :] + r1[j, keep, :].astype(F32)

    def second_matmul_to_all(j):
        arrived(h_buf.at[pl.ds(0, 3), pl.ds(0, TC), :], HY + j)
        sd[pl.ds((1 - b0) * 4, 4)] = times_hidden((1 - b0) * 256, j).astype(BF16).reshape(4, 64, TC)
        for m in (7, 5, 3, 1):
            to, at = z_mate(m)
            send(sd.at[at], rd.at[place], RS + 3 * j, to, S_L)
        kd[...] = times_hidden(b0 * 256, j).reshape(4, 64, TC)
        for m in (6, 4, 2):
            to, at = z_mate(m)
            sd[at] = kd[at % 4].astype(BF16)
            send(sd.at[at], rd.at[place], RS + 3 * j, to, S_L)

    def next_step(j):
        if STEPS[j] == 3:
            halve(j)
        elif STEPS[j] == 2:
            halve_and_send(j)

    for j in range(NT):
        if STEPS[j] == 1:
            second_matmul_to_all(j)
        else:
            second_matmul(j)
        if j >= 2:
            next_step(j - 2)
    next_step(NT - 2)
    next_step(NT - 1)
    for j in [j for j in range(NT) if STEPS[j] == 3]:
        arrived(r2.at[j], RS + 3 * j + 1)
        out, keep = aligned((1 - b2) * 64, 64), aligned(b2 * 64, 64)
        s3[j] = (k2[j, out, :] + r2[j, out, :].astype(F32)).astype(BF16)
        send(s3.at[j], r3.at[j], RS + 3 * j + 2, to_z4, S_L)
        k3[j] = k2[j, keep, :] + r2[j, keep, :].astype(F32)

    dn_over_core(0)
    dn_over_core(1)

    arrived(dn_buf.at[:, pl.ds(0, D // 2)], DNC)

    for j in range(NT):
        if STEPS[j] == 3:
            arrived(r3.at[j], RS + 3 * j + 2)
            total = k3[j] + r3[j].astype(F32)
        elif STEPS[j] == 2:
            arrived(rm.at[j, pl.ds(0, 3)], RS + 3 * j + 1)
            total = k3[j]
            for m in (2, 4, 6):
                total += rm[j, z_mate(m)[1] % 4].astype(F32)
        else:
            arrived(rd.at[pl.ds(0, 7)], RS + 3 * j)
            total = kd[place % 4]
            for m in range(1, 8):
                total += rd[z_mate(m)[1]].astype(F32)
        mix_ref[:, j * TC : (j + 1) * TC] = total.astype(BF16)

    all_left(S_W, (64 + 384 + 512 + 64 + 384 + 512) * KIB)
    all_left(S_L, (768 + NT * 112) * KIB)

    @pl.when(g == 1)
    def _():
        all_left(S_G, 64 * KIB)

    @pl.when(relays)
    def _():
        all_left(S_R, 128 * KIB)

    @pl.when(owner)
    def _():
        all_left(S_Y, 64 * KIB)
        all_left(S_X, 2 * 7 * 128 * KIB)

    @pl.when(jnp.logical_not(owner))
    def _():
        all_left(S_Y, 128 * KIB)


def write_out(up_ref, dn_ref, mix_ref, up_hbm, dn_hbm, mix_hbm, lsem):
    copies = [
        pltpu.make_async_copy(src, dst, lsem.at[i])
        for i, (src, dst) in enumerate(((up_ref, up_hbm), (dn_ref, dn_hbm), (mix_ref, mix_hbm)))
    ]
    for copy in copies:
        copy.start()
    for copy in copies:
        copy.wait()


def per_device(tokens, norm_gain, up_weight, down_weight):
    hbm = pl.BlockSpec(memory_space=pltpu.HBM)
    vmem = pl.BlockSpec(memory_space=pltpu.VMEM)
    up_block, down_block, mixed = pl.pallas_call(
        kernel,
        out_shape=(
            jax.ShapeDtypeStruct((D, UNITS), BF16),
            jax.ShapeDtypeStruct((UNITS, D), BF16),
            jax.ShapeDtypeStruct((64, TOK), BF16),
        ),
        in_specs=[hbm] * 4,
        out_specs=(vmem,) * 3,
        scratch_shapes=[
            pltpu.VMEM((1, 64), F32),
            pltpu.VMEM((64, 512), F32),
            pltpu.VMEM((256, 128), F32),
            pltpu.VMEM((2, 64, 256), BF16),
            pltpu.VMEM((2, 2, 64, 256), BF16),
            pltpu.VMEM((4, 512, 256), BF16),
            pltpu.VMEM((TOK, D), BF16),
            pltpu.VMEM((4, TOK, UNITS), BF16),
            pltpu.VMEM((NT, 256, TC), BF16),
            pltpu.VMEM((NT, 256, TC), BF16),
            pltpu.VMEM((NT, 256, TC), F32),
            pltpu.VMEM((NT, 128, TC), BF16),
            pltpu.VMEM((NT, 128, TC), BF16),
            pltpu.VMEM((NT, 128, TC), F32),
            pltpu.VMEM((NT, 64, TC), BF16),
            pltpu.VMEM((NT, 64, TC), BF16),
            pltpu.VMEM((NT, 64, TC), F32),
            pltpu.VMEM((NT, 4, 64, TC), BF16),
            pltpu.VMEM((NT, 4, 64, TC), BF16),
            pltpu.VMEM((8, 64, TC), BF16),
            pltpu.VMEM((8, 64, TC), BF16),
            pltpu.VMEM((4, 64, TC), F32),
            pltpu.SemaphoreType.DMA((N_SEND,)),
            pltpu.SemaphoreType.DMA((N_RECV,)),
            pltpu.SemaphoreType.DMA((4,)),
            pltpu.SemaphoreType.REGULAR,
        ],
        compiler_params=pltpu.CompilerParams(
            collective_id=0, has_side_effects=True, vmem_limit_bytes=16 * 1024 * 1024
        ),
        name="handoff",
    )(*(
        pltpu.with_memory_space_constraint(a, pltpu.HBM)
        for a in (tokens, norm_gain.reshape(1, 64), up_weight, down_weight)
    ))
    results = (up_block, down_block, mixed)
    up_block, down_block, mixed = pl.pallas_call(
        write_out,
        out_shape=tuple(jax.ShapeDtypeStruct(a.shape, a.dtype) for a in results),
        in_specs=[vmem] * 3,
        out_specs=(hbm,) * 3,
        scratch_shapes=[pltpu.SemaphoreType.DMA((3,))],
        compiler_params=pltpu.CompilerParams(vmem_limit_bytes=8 * 1024 * 1024),
        name="write_out",
    )(*results)
    return up_block, down_block, mixed.T


def solution(mesh):
    in_specs = (P(("gr", "tp"), None), P("fs"), P("fs", ("gr", "tp")), P("fs", ("gr", "tp")))
    out_specs = (P(None, "fs"), P("fs", None), P(("gr", "tp"), "fs"))
    return jax.shard_map(
        per_device, mesh=mesh, in_specs=in_specs, out_specs=out_specs, check_vma=False
    )
```

```python
import jax
import jax.numpy as jnp
from jax import lax
from jax.experimental import pallas as pl
from jax.experimental.pallas import tpu as pltpu
from jax.sharding import PartitionSpec as P

MESH = pl.DeviceIdType.MESH
F32 = jnp.float32
BF16 = jnp.bfloat16

TOK = 512
D = 2048
UNITS = 256
HALF = 128
NT = 4
TC = TOK // NT
STEPS = (3, 3, 2, 2)
NORM_U, NORM_A, NORM_B = 18, 24, 32


def numbered(*sizes):
    firsts, at = [], 0
    for size in sizes:
        firsts.append(at)
        at += size
    return (*firsts, at)


UP1, UPF, UPX, UPC, DNG, DNX, DNC, DTY, DTX, DTC, HY, RS, N_RECV = numbered(
    4, 4, 12, 2, 1, 2, 1, 2, 6, 1, NT, 3 * NT
)
S_W, S_L, S_G, S_R, S_Y, S_X, N_SEND = numbered(1, 1, 1, 1, 1, 1)
KIB = 1024
MATES = tuple(range(1, 8)) if 1 in STEPS else (1, 2, 4, 6) if 2 in STEPS else (1, 2, 4)


def kernel(
    tok_hbm, gain_hbm, upw_hbm, dnw_hbm,
    up_buf, dn_buf, mix_ref,
    gain_ref, upw_ref, dnw_ref,
    u_send, dt_send, dt_buf, nrm, h_buf,
    s1, r1, k1, s2, r2, k2, s3, r3, k3,
    sm, rm, sd, rd, kd,
    ssem, rsem, lsem, far_sem,
):
    g = lax.axis_index("gr")
    f = lax.axis_index("fs")
    t = lax.axis_index("tp")
    zl, y = f // 4, f % 4
    x, k = t // 2, t % 2
    ok = 1 - k
    og = 1 - g

    def dev(gg, zz, yy, xx, kk):
        return (gg, zz * 4 + yy, xx * 2 + kk)

    def message(src, dst, i, to, group):
        return pltpu.make_async_remote_copy(
            src_ref=src, dst_ref=dst, send_sem=ssem.at[group], recv_sem=rsem.at[i],
            device_id=to, device_id_type=MESH,
        )

    def send(src, dst, i, to, group=S_W):
        message(src, dst, i, to, group).start()

    to_core = dev(g, zl, y, x, ok)

    def arrived(landed, i):
        message(landed, landed, i, to_core, S_W).wait_recv()

    def all_left(group, size):
        rows = nrm.at[pl.ds(0, size // (2 * D)), :]
        message(rows, rows, 0, to_core, group).wait_send()

    steps = (2, 1, 3)
    x_to = [dev(g, zl, y, (x + s) % 4, k) for s in steps]
    x_from = [(x + 4 - s) % 4 for s in steps]
    y_to = [dev(g, zl, (y + s) % 4, x, k) for s in steps]
    y_from = [(y + 4 - s) % 4 for s in steps]
    b0, b1, b2 = zl % 2, (zl // 2) % 2, zl // 4
    to_z1 = dev(g, zl + 1 - 2 * b0, y, x, k)
    to_z2 = dev(g, zl + 2 - 4 * b1, y, x, k)
    to_z4 = dev(g, zl + 4 - 8 * b2, y, x, k)
    to_gr = dev(og, zl, y, x, k)

    place = b0 * 4 + b1 * 2 + b2

    def z_mate(m):
        flip = [abs(b - (m >> i) % 2) for i, b in enumerate((b0, b1, b2))]
        return dev(g, flip[0] + 2 * flip[1] + 4 * flip[2], y, x, k), flip[0] * 4 + flip[1] * 2 + flip[2]


    xs, ks, hs = zl % 4, y // 2, y % 2
    relayed = jnp.logical_and(g == 1, b2 == 0)
    relays = jnp.logical_and(g == 0, b2 == 0)

    def a_of(xx):
        return (xx - xs - hs - 2 * g * b2 + 8) % 4

    a_me = a_of(x)
    sources = [
        (q * 2 + w, dev(b2, a_me + 4 * q, 2 * ok + w, xs, ks)) for q in range(2) for w in range(2)
    ]

    barrier = pltpu.get_barrier_semaphore()

    def greet(who):
        pl.semaphore_signal(barrier, inc=1, device_id=who, device_id_type=MESH)

    @pl.when(jnp.logical_not(relayed))
    def _():
        for _, source in sources:
            greet(source)

    @pl.when(g == 0)
    def _():
        greet(to_gr)

    for who in (*x_to, *y_to, to_core, *(z_mate(m)[0] for m in MATES)):
        greet(who)

    loads = [
        pltpu.make_async_copy(src, dst, lsem.at[i])
        for i, (src, dst) in enumerate(
            ((gain_hbm, gain_ref), (upw_hbm, upw_ref), (dnw_hbm, dnw_ref), (tok_hbm, nrm))
        )
    ]
    for load in loads:
        load.start()

    loads[0].wait()
    loads[1].wait()
    rows = lax.broadcasted_iota(jnp.int32, (64, 64), 0)
    cols = lax.broadcasted_iota(jnp.int32, (64, 64), 1)
    gain_wide = jnp.broadcast_to(gain_ref[...], (64, 64))
    gain = jnp.sum(jnp.where(rows == cols, gain_wide, 0.0), axis=1, keepdims=True)
    for h in range(2):
        u_send[h] = (gain * upw_ref[:, h * 256 : (h + 1) * 256]).astype(BF16)

    def dn_cols(gg, xx, kk):
        return pl.ds(pl.multiple_of((gg * 8 + xx * 2 + kk) * 128, 128), 128)

    def dn_piece(gg, xx, kk):
        return dn_buf.at[:, dn_cols(gg, xx, kk)]

    loads[2].wait()
    dn_mine = dnw_ref[...]
    dn_buf[:, dn_cols(g, x, k)] = dn_mine.astype(BF16)

    dt_mine = dn_mine.T.astype(BF16)
    for h in range(2):
        dt_send[0, h] = dt_mine[h * 64 : (h + 1) * 64]

    @pl.when(g == 0)
    def _():
        pl.semaphore_wait(barrier, 9 + len(MATES))

    @pl.when(g == 1)
    def _():
        pl.semaphore_wait(barrier, 12 + len(MATES))
        pl.semaphore_signal(far_sem, inc=1, device_id=to_gr, device_id_type=MESH)


    def up_piece(xx, q, kk, u):
        start = ((a_of(xx) + 4 * q) * 4 + 2 * (1 - kk)) * 64
        return up_buf.at[pl.ds(pl.multiple_of(start, 128), 128), pl.ds(u * HALF, HALF)]

    def up_message(u, gg, h):
        xx = (x + zl + h + 2 * gg) % 4
        to = (gg, (4 * g + x) * 4 + 2 * k + h, xx * 2 + (1 - y // 2))
        slot = up_buf.at[pl.ds(pl.multiple_of(f * 64, 64), 64), pl.ds(u * HALF, HALF)]
        src = u_send.at[h, :, pl.ds(u * HALF, HALF)]
        return message(src, slot, UP1 + u * 2 + b2, to, (S_W, S_G)[gg])

    def up_first(u):
        for h in range(2):
            up_message(u, 0, h).start()

        @pl.when(g == 1)
        def _():
            for h in range(2):
                up_message(u, 1, h).start()

    def up_relay(u, q):
        piece = up_piece(x, q, k, u)
        return message(piece, piece, UPF + u * 2 + q, to_gr, S_R)

    up_first(0)

    owner = ks == k
    halves = (g, og)

    def dt_rows(part, xx):
        return pl.ds(pl.multiple_of(((xx % 2) * 4 + (xx // 2) * 2 + halves[part]) * 64, 64), 64)

    def dt_piece(part, xx):
        return dt_buf.at[:, dt_rows(part, xx), :]

    def dt_to_y(part, h):
        return message(
            dt_send.at[part, h], dt_buf.at[y, dt_rows(part, x), :],
            DTY + part, dev(g, zl, 2 * k + h, x, k), S_Y,
        )

    def dt_over_y(part):
        for h in range(2):

            @pl.when(2 * k + h != y)
            def _():
                dt_to_y(part, h).start()

            @pl.when(2 * k + h == y)
            def _():
                dt_buf[y, dt_rows(part, x), :] = dt_send[part, h]

    def dt_from_x(part):
        piece = dt_piece(part, x)
        return [message(piece, piece, DTX + part * 3 + d, x_to[d], S_X) for d in range(3)] + [
            message(piece, piece, DTC, to_core, S_X)
        ]

    def dt_over_x(part):
        @pl.when(owner)
        def _():
            arrived(dt_buf.at[pl.ds(0, 3), dt_rows(part, x), :], DTY + part)
            for copy in dt_from_x(part):
                copy.start()

    def dt_to_core(part, d):
        piece = dt_piece(part, x_from[d])
        return message(piece, piece, DTC, to_core, S_X)

    def dt_over_core(part):
        @pl.when(owner)
        def _():
            for d in (1, 2, 0):
                arrived(dt_piece(part, x_from[d]), DTX + part * 3 + d)
                dt_to_core(part, d).start()

    def dn_over_x(part):
        piece = dn_piece(halves[part], x, k)
        for d in range(3):
            send(piece, piece, DNX + part, x_to[d])
        send(piece, piece, DNC, to_core)

    def dn_over_core(part):
        arrived(dn_buf.at[:, pl.ds(0, 3 * 128)], DNX + part)
        for d in range(3):
            piece = dn_piece(halves[part], x_from[d], k)
            send(piece, piece, DNC, to_core)

    dt_over_y(0)
    dn_over_x(0)

    loads[3].wait()

    def norm_rows(i, _):
        at = pl.ds(pl.multiple_of(i * 16, 16), 16)
        wide = nrm[at, :].astype(F32)
        scale = lax.rsqrt(jnp.mean(wide * wide, axis=-1, keepdims=True) + 1e-06)
        nrm[at, :] = (wide * scale).astype(BF16)
        return 0

    lax.fori_loop(0, NORM_U, norm_rows, 0)
    up_first(1)
    lax.fori_loop(NORM_U, NORM_A, norm_rows, 0)
    dt_over_x(0)
    lax.fori_loop(NORM_A, NORM_B, norm_rows, 0)
    lax.fori_loop(NORM_B, TOK // 16, norm_rows, 0)

    @pl.when(g == 0)
    def _():
        pl.semaphore_wait(far_sem, 1)

    def up_in(u):
        for q in range(2):

            @pl.when(relayed)
            def _():
                arrived(up_piece(x, q, k, u), UPF + u * 2 + q)

            @pl.when(jnp.logical_not(relayed))
            def _():
                arrived(up_piece(x, q, k, u), UP1 + u * 2 + q)

            @pl.when(relays)
            def _():
                up_relay(u, q).start()

            piece = up_piece(x, q, k, u)
            for d in (1, 2, 0):
                send(piece, piece, UPX + u * 6 + q * 3 + d, x_to[d])
            send(piece, piece, UPC + u, to_core)

    send(dn_piece(g, x, k), dn_piece(g, x, k), DNG, to_gr)
    up_in(0)
    up_in(1)

    def up_to_core(u):
        for d in (1, 2, 0):
            for q in range(2):
                piece = up_piece(x_from[d], q, k, u)
                arrived(piece, UPX + u * 6 + q * 3 + d)
                send(piece, piece, UPC + u, to_core)

    def hidden_out(u, j):
        piece = h_buf.at[y, pl.ds(j * TC, TC), pl.ds(u * HALF, HALF)]
        for d in (1, 2, 0):
            send(piece, piece, HY + j, y_to[d], S_L)

    def hidden_half(u, order):
        arrived(up_buf.at[pl.ds(0, D // 2), pl.ds(u * HALF, HALF)], UPC + u)
        units = pl.ds(u * HALF, HALF)
        for part in range(2):
            at = pl.ds(part * TOK // 2, TOK // 2)
            pre = jnp.dot(nrm[at, :], up_buf[:, units], preferred_element_type=F32)
            pre = jnp.maximum(pre, 0.0)
            h_buf[y, at, units] = (pre * pre).astype(BF16)
            for uu, j in order[part]:
                hidden_out(uu, j)

    dt_over_core(0)
    up_to_core(0)
    arrived(dn_piece(og, x, k), DNG)
    dt_other = dn_buf[:, dn_cols(og, x, k)].astype(F32).T.astype(BF16)
    for h in range(2):
        dt_send[1, h] = dt_other[h * 64 : (h + 1) * 64]
    dt_over_y(1)

    hidden_half(0, (((0, 0), (0, 1)), ((0, 2),)))

    dt_over_x(1)
    up_to_core(1)
    hidden_half(1, (((1, 0), (1, 1)), ((1, 2), (0, 3), (1, 3))))

    dn_over_x(1)

    dt_over_core(1)

    @pl.when(jnp.logical_not(owner))
    def _():
        arrived(dt_buf, DTC)

    def times_hidden(first, j):
        rows_at = pl.ds(pl.multiple_of(first, 256), 256)
        total = jnp.zeros((256, TC), F32)
        for yy in range(4):
            total += lax.dot_general(
                dt_buf[yy, rows_at, :], h_buf[yy, pl.ds(j * TC, TC), :],
                (((1,), (1,)), ((), ())), preferred_element_type=F32,
            )
        return total

    def aligned(start, size):
        return pl.ds(pl.multiple_of(start, 64), size)

    def second_matmul(j):
        arrived(h_buf.at[pl.ds(0, 3), pl.ds(0, TC), :], HY + j)
        s1[j] = times_hidden((1 - b0) * 256, j).astype(BF16)
        send(s1.at[j], r1.at[j], RS + 3 * j, to_z1, S_L)
        k1[j] = times_hidden(b0 * 256, j)

    def halve(j):
        arrived(r1.at[j], RS + 3 * j)
        out, keep = aligned((1 - b1) * 128, 128), aligned(b1 * 128, 128)
        s2[j] = (k1[j, out, :] + r1[j, out, :].astype(F32)).astype(BF16)
        send(s2.at[j], r2.at[j], RS + 3 * j + 1, to_z2, S_L)
        k2[j] = k1[j, keep, :] + r1[j, keep, :].astype(F32)

    def halve_and_send(j):
        arrived(r1.at[j], RS + 3 * j)
        half_place = b1 * 2 + b2
        for m in (6, 4, 2):
            to, at_place = z_mate(m)
            at = at_place % 4
            rows_at = aligned(at * 64, 64)
            sm[j, at] = (k1[j, rows_at, :] + r1[j, rows_at, :].astype(F32)).astype(BF16)
            send(sm.at[j, at], rm.at[j, half_place], RS + 3 * j + 1, to, S_L)
        keep = aligned(half_place * 64, 64)
        k3[j] = k1[j, keep, :] + r1[j, keep, :].astype(F32)

    def second_matmul_to_all(j):
        arrived(h_buf.at[pl.ds(0, 3), pl.ds(0, TC), :], HY + j)
        sd[pl.ds((1 - b0) * 4, 4)] = times_hidden((1 - b0) * 256, j).astype(BF16).reshape(4, 64, TC)
        for m in (7, 5, 3, 1):
            to, at = z_mate(m)
            send(sd.at[at], rd.at[place], RS + 3 * j, to, S_L)
        kd[...] = times_hidden(b0 * 256, j).reshape(4, 64, TC)
        for m in (6, 4, 2):
            to, at = z_mate(m)
            sd[at] = kd[at % 4].astype(BF16)
            send(sd.at[at], rd.at[place], RS + 3 * j, to, S_L)

    def next_step(j):
        if STEPS[j] == 3:
            halve(j)
        elif STEPS[j] == 2:
            halve_and_send(j)

    for j in range(NT):
        if STEPS[j] == 1:
            second_matmul_to_all(j)
        else:
            second_matmul(j)
        if j >= 2:
            next_step(j - 2)
    next_step(NT - 2)
    next_step(NT - 1)
    for j in [j for j in range(NT) if STEPS[j] == 3]:
        arrived(r2.at[j], RS + 3 * j + 1)
        out, keep = aligned((1 - b2) * 64, 64), aligned(b2 * 64, 64)
        s3[j] = (k2[j, out, :] + r2[j, out, :].astype(F32)).astype(BF16)
        send(s3.at[j], r3.at[j], RS + 3 * j + 2, to_z4, S_L)
        k3[j] = k2[j, keep, :] + r2[j, keep, :].astype(F32)

    dn_over_core(0)
    dn_over_core(1)

    arrived(dn_buf.at[:, pl.ds(0, D // 2)], DNC)

    for j in range(NT):
        if STEPS[j] == 3:
            arrived(r3.at[j], RS + 3 * j + 2)
            total = k3[j] + r3[j].astype(F32)
        elif STEPS[j] == 2:
            arrived(rm.at[j, pl.ds(0, 3)], RS + 3 * j + 1)
            total = k3[j]
            for m in (2, 4, 6):
                total += rm[j, z_mate(m)[1] % 4].astype(F32)
        else:
            arrived(rd.at[pl.ds(0, 7)], RS + 3 * j)
            total = kd[place % 4]
            for m in range(1, 8):
                total += rd[z_mate(m)[1]].astype(F32)
        mix_ref[:, j * TC : (j + 1) * TC] = total.astype(BF16)

    all_left(S_W, (64 + 384 + 512 + 64 + 384 + 512) * KIB)
    all_left(S_L, (768 + NT * 112) * KIB)

    @pl.when(g == 1)
    def _():
        all_left(S_G, 64 * KIB)

    @pl.when(relays)
    def _():
        all_left(S_R, 128 * KIB)

    @pl.when(owner)
    def _():
        all_left(S_Y, 64 * KIB)
        all_left(S_X, 2 * 7 * 128 * KIB)

    @pl.when(jnp.logical_not(owner))
    def _():
        all_left(S_Y, 128 * KIB)


def write_out(up_ref, dn_ref, mix_ref, up_hbm, dn_hbm, mix_hbm, lsem):
    copies = [
        pltpu.make_async_copy(src, dst, lsem.at[i])
        for i, (src, dst) in enumerate(((up_ref, up_hbm), (dn_ref, dn_hbm), (mix_ref, mix_hbm)))
    ]
    for copy in copies:
        copy.start()
    for copy in copies:
        copy.wait()


def per_device(tokens, norm_gain, up_weight, down_weight):
    hbm = pl.BlockSpec(memory_space=pltpu.HBM)
    vmem = pl.BlockSpec(memory_space=pltpu.VMEM)
    up_block, down_block, mixed = pl.pallas_call(
        kernel,
        out_shape=(
            jax.ShapeDtypeStruct((D, UNITS), BF16),
            jax.ShapeDtypeStruct((UNITS, D), BF16),
            jax.ShapeDtypeStruct((64, TOK), BF16),
        ),
        in_specs=[hbm] * 4,
        out_specs=(vmem,) * 3,
        scratch_shapes=[
            pltpu.VMEM((1, 64), F32),
            pltpu.VMEM((64, 512), F32),
            pltpu.VMEM((256, 128), F32),
            pltpu.VMEM((2, 64, 256), BF16),
            pltpu.VMEM((2, 2, 64, 256), BF16),
            pltpu.VMEM((4, 512, 256), BF16),
            pltpu.VMEM((TOK, D), BF16),
            pltpu.VMEM((4, TOK, UNITS), BF16),
            pltpu.VMEM((NT, 256, TC), BF16),
            pltpu.VMEM((NT, 256, TC), BF16),
            pltpu.VMEM((NT, 256, TC), F32),
            pltpu.VMEM((NT, 128, TC), BF16),
            pltpu.VMEM((NT, 128, TC), BF16),
            pltpu.VMEM((NT, 128, TC), F32),
            pltpu.VMEM((NT, 64, TC), BF16),
            pltpu.VMEM((NT, 64, TC), BF16),
            pltpu.VMEM((NT, 64, TC), F32),
            pltpu.VMEM((NT, 4, 64, TC), BF16),
            pltpu.VMEM((NT, 4, 64, TC), BF16),
            pltpu.VMEM((8, 64, TC), BF16),
            pltpu.VMEM((8, 64, TC), BF16),
            pltpu.VMEM((4, 64, TC), F32),
            pltpu.SemaphoreType.DMA((N_SEND,)),
            pltpu.SemaphoreType.DMA((N_RECV,)),
            pltpu.SemaphoreType.DMA((4,)),
            pltpu.SemaphoreType.REGULAR,
        ],
        compiler_params=pltpu.CompilerParams(
            collective_id=0, has_side_effects=True, vmem_limit_bytes=16 * 1024 * 1024
        ),
        name="handoff",
    )(*(
        pltpu.with_memory_space_constraint(a, pltpu.HBM)
        for a in (tokens, norm_gain.reshape(1, 64), up_weight, down_weight)
    ))
    results = (up_block, down_block, mixed)
    up_block, down_block, mixed = pl.pallas_call(
        write_out,
        out_shape=tuple(jax.ShapeDtypeStruct(a.shape, a.dtype) for a in results),
        in_specs=[vmem] * 3,
        out_specs=(hbm,) * 3,
        scratch_shapes=[pltpu.SemaphoreType.DMA((3,))],
        compiler_params=pltpu.CompilerParams(vmem_limit_bytes=8 * 1024 * 1024),
        name="write_out",
    )(*results)
    return up_block, down_block, mixed.T


def solution(mesh):
    in_specs = (P(("gr", "tp"), None), P("fs"), P("fs", ("gr", "tp")), P("fs", ("gr", "tp")))
    out_specs = (P(None, "fs"), P("fs", None), P(("gr", "tp"), "fs"))
    return jax.shard_map(
        per_device, mesh=mesh, in_specs=in_specs, out_specs=out_specs, check_vma=False
    )
```

```python
import jax
import jax.numpy as jnp
from jax import lax
from jax.experimental import pallas as pl
from jax.experimental.pallas import tpu as pltpu
from jax.sharding import PartitionSpec as P

MESH = pl.DeviceIdType.MESH
F32 = jnp.float32
BF16 = jnp.bfloat16

TOK = 512
D = 2048
UNITS = 256
HALF = 128
NT = 4
TC = TOK // NT
STEPS = (3, 3, 2, 2)
NORM_U, NORM_A, NORM_B = 18, 24, 32


def numbered(*sizes):
    firsts, at = [], 0
    for size in sizes:
        firsts.append(at)
        at += size
    return (*firsts, at)


UP1, UPF, UPX, UPC, DNG, DNX, DNC, DTY, DTX, DTC, HY, RS, N_RECV = numbered(
    4, 4, 12, 2, 1, 2, 1, 2, 6, 1, NT, 3 * NT
)
S_W, S_L, S_G, S_R, S_Y, S_X, N_SEND = numbered(1, 1, 1, 1, 1, 1)
KIB = 1024
MATES = tuple(range(1, 8)) if 1 in STEPS else (1, 2, 4, 6) if 2 in STEPS else (1, 2, 4)


def kernel(
    tok_hbm, gain_hbm, upw_hbm, dnw_hbm,
    up_buf, dn_buf, mix_ref,
    gain_ref, upw_ref, dnw_ref,
    u_send, dt_send, dt_buf, nrm, h_buf,
    s1, r1, k1, s2, r2, k2, s3, r3, k3,
    sm, rm, sd, rd, kd,
    ssem, rsem, lsem, far_sem,
):
    g = lax.axis_index("gr")
    f = lax.axis_index("fs")
    t = lax.axis_index("tp")
    zl, y = f // 4, f % 4
    x, k = t // 2, t % 2
    ok = 1 - k
    og = 1 - g

    def dev(gg, zz, yy, xx, kk):
        return (gg, zz * 4 + yy, xx * 2 + kk)

    def message(src, dst, i, to, group):
        return pltpu.make_async_remote_copy(
            src_ref=src, dst_ref=dst, send_sem=ssem.at[group], recv_sem=rsem.at[i],
            device_id=to, device_id_type=MESH,
        )

    def send(src, dst, i, to, group=S_W):
        message(src, dst, i, to, group).start()

    to_core = dev(g, zl, y, x, ok)

    def arrived(landed, i):
        message(landed, landed, i, to_core, S_W).wait_recv()

    def all_left(group, size):
        rows = nrm.at[pl.ds(0, size // (2 * D)), :]
        message(rows, rows, 0, to_core, group).wait_send()

    steps = (2, 1, 3)
    x_to = [dev(g, zl, y, (x + s) % 4, k) for s in steps]
    x_from = [(x + 4 - s) % 4 for s in steps]
    y_to = [dev(g, zl, (y + s) % 4, x, k) for s in steps]
    y_from = [(y + 4 - s) % 4 for s in steps]
    b0, b1, b2 = zl % 2, (zl // 2) % 2, zl // 4
    to_z1 = dev(g, zl + 1 - 2 * b0, y, x, k)
    to_z2 = dev(g, zl + 2 - 4 * b1, y, x, k)
    to_z4 = dev(g, zl + 4 - 8 * b2, y, x, k)
    to_gr = dev(og, zl, y, x, k)

    place = b0 * 4 + b1 * 2 + b2

    def z_mate(m):
        flip = [abs(b - (m >> i) % 2) for i, b in enumerate((b0, b1, b2))]
        return dev(g, flip[0] + 2 * flip[1] + 4 * flip[2], y, x, k), flip[0] * 4 + flip[1] * 2 + flip[2]


    xs, ks, hs = zl % 4, y // 2, y % 2
    relayed = jnp.logical_and(g == 1, b2 == 0)
    relays = jnp.logical_and(g == 0, b2 == 0)

    def a_of(xx):
        return (xx - xs - hs - 2 * g * b2 + 8) % 4

    a_me = a_of(x)
    sources = [
        (q * 2 + w, dev(b2, a_me + 4 * q, 2 * ok + w, xs, ks)) for q in range(2) for w in range(2)
    ]

    barrier = pltpu.get_barrier_semaphore()

    def greet(who):
        pl.semaphore_signal(barrier, inc=1, device_id=who, device_id_type=MESH)

    @pl.when(jnp.logical_not(relayed))
    def _():
        for _, source in sources:
            greet(source)

    @pl.when(g == 0)
    def _():
        greet(to_gr)

    for who in (*x_to, *y_to, to_core, *(z_mate(m)[0] for m in MATES)):
        greet(who)

    loads = [
        pltpu.make_async_copy(src, dst, lsem.at[i])
        for i, (src, dst) in enumerate(
            ((gain_hbm, gain_ref), (upw_hbm, upw_ref), (dnw_hbm, dnw_ref), (tok_hbm, nrm))
        )
    ]
    for load in loads:
        load.start()

    loads[0].wait()
    loads[1].wait()
    rows = lax.broadcasted_iota(jnp.int32, (64, 64), 0)
    cols = lax.broadcasted_iota(jnp.int32, (64, 64), 1)
    gain_wide = jnp.broadcast_to(gain_ref[...], (64, 64))
    gain = jnp.sum(jnp.where(rows == cols, gain_wide, 0.0), axis=1, keepdims=True)
    for h in range(2):
        u_send[h] = (gain * upw_ref[:, h * 256 : (h + 1) * 256]).astype(BF16)

    def dn_cols(gg, xx, kk):
        return pl.ds(pl.multiple_of((gg * 8 + xx * 2 + kk) * 128, 128), 128)

    def dn_piece(gg, xx, kk):
        return dn_buf.at[:, dn_cols(gg, xx, kk)]

    loads[2].wait()
    dn_mine = dnw_ref[...]
    dn_buf[:, dn_cols(g, x, k)] = dn_mine.astype(BF16)

    dt_mine = dn_mine.T.astype(BF16)
    for h in range(2):
        dt_send[0, h] = dt_mine[h * 64 : (h + 1) * 64]

    @pl.when(g == 0)
    def _():
        pl.semaphore_wait(barrier, 9 + len(MATES))

    @pl.when(g == 1)
    def _():
        pl.semaphore_wait(barrier, 12 + len(MATES))
        pl.semaphore_signal(far_sem, inc=1, device_id=to_gr, device_id_type=MESH)


    def up_piece(xx, q, kk, u):
        start = ((a_of(xx) + 4 * q) * 4 + 2 * (1 - kk)) * 64
        return up_buf.at[pl.ds(pl.multiple_of(start, 128), 128), pl.ds(u * HALF, HALF)]

    def up_message(u, gg, h):
        xx = (x + zl + h + 2 * gg) % 4
        to = (gg, (4 * g + x) * 4 + 2 * k + h, xx * 2 + (1 - y // 2))
        slot = up_buf.at[pl.ds(pl.multiple_of(f * 64, 64), 64), pl.ds(u * HALF, HALF)]
        src = u_send.at[h, :, pl.ds(u * HALF, HALF)]
        return message(src, slot, UP1 + u * 2 + b2, to, (S_W, S_G)[gg])

    def up_first(u):
        for h in range(2):
            up_message(u, 0, h).start()

        @pl.when(g == 1)
        def _():
            for h in range(2):
                up_message(u, 1, h).start()

    def up_relay(u, q):
        piece = up_piece(x, q, k, u)
        return message(piece, piece, UPF + u * 2 + q, to_gr, S_R)

    up_first(0)

    owner = ks == k
    halves = (g, og)

    def dt_rows(part, xx):
        return pl.ds(pl.multiple_of(((xx % 2) * 4 + (xx // 2) * 2 + halves[part]) * 64, 64), 64)

    def dt_piece(part, xx):
        return dt_buf.at[:, dt_rows(part, xx), :]

    def dt_to_y(part, h):
        return message(
            dt_send.at[part, h], dt_buf.at[y, dt_rows(part, x), :],
            DTY + part, dev(g, zl, 2 * k + h, x, k), S_Y,
        )

    def dt_over_y(part):
        for h in range(2):

            @pl.when(2 * k + h != y)
            def _():
                dt_to_y(part, h).start()

            @pl.when(2 * k + h == y)
            def _():
                dt_buf[y, dt_rows(part, x), :] = dt_send[part, h]

    def dt_from_x(part):
        piece = dt_piece(part, x)
        return [message(piece, piece, DTX + part * 3 + d, x_to[d], S_X) for d in (1, 2, 0)] + [
            message(piece, piece, DTC, to_core, S_X)
        ]

    def dt_over_x(part):
        @pl.when(owner)
        def _():
            arrived(dt_buf.at[pl.ds(0, 3), dt_rows(part, x), :], DTY + part)
            for copy in dt_from_x(part):
                copy.start()

    def dt_to_core(part, d):
        piece = dt_piece(part, x_from[d])
        return message(piece, piece, DTC, to_core, S_X)

    def dt_over_core(part):
        @pl.when(owner)
        def _():
            for d in (1, 2, 0):
                arrived(dt_piece(part, x_from[d]), DTX + part * 3 + d)
                dt_to_core(part, d).start()

    def dn_over_x(part):
        piece = dn_piece(halves[part], x, k)
        for d in (1, 2, 0):
            send(piece, piece, DNX + part, x_to[d])
        send(piece, piece, DNC, to_core)

    def dn_over_core(part):
        arrived(dn_buf.at[:, pl.ds(0, 3 * 128)], DNX + part)
        for d in range(3):
            piece = dn_piece(halves[part], x_from[d], k)
            send(piece, piece, DNC, to_core)

    dt_over_y(0)
    dn_over_x(0)

    loads[3].wait()

    def norm_rows(i, _):
        at = pl.ds(pl.multiple_of(i * 16, 16), 16)
        wide = nrm[at, :].astype(F32)
        scale = lax.rsqrt(jnp.mean(wide * wide, axis=-1, keepdims=True) + 1e-06)
        nrm[at, :] = (wide * scale).astype(BF16)
        return 0

    lax.fori_loop(0, NORM_U, norm_rows, 0)
    up_first(1)
    lax.fori_loop(NORM_U, NORM_A, norm_rows, 0)
    dt_over_x(0)
    lax.fori_loop(NORM_A, NORM_B, norm_rows, 0)
    lax.fori_loop(NORM_B, TOK // 16, norm_rows, 0)

    @pl.when(g == 0)
    def _():
        pl.semaphore_wait(far_sem, 1)

    def up_in(u):
        for q in range(2):

            @pl.when(relayed)
            def _():
                arrived(up_piece(x, q, k, u), UPF + u * 2 + q)

            @pl.when(jnp.logical_not(relayed))
            def _():
                arrived(up_piece(x, q, k, u), UP1 + u * 2 + q)

            @pl.when(relays)
            def _():
                up_relay(u, q).start()

            piece = up_piece(x, q, k, u)
            for d in (1, 2, 0):
                send(piece, piece, UPX + u * 6 + q * 3 + d, x_to[d])
            send(piece, piece, UPC + u, to_core)

    send(dn_piece(g, x, k), dn_piece(g, x, k), DNG, to_gr)
    up_in(0)
    up_in(1)

    def up_to_core(u):
        for d in (1, 2, 0):
            for q in range(2):
                piece = up_piece(x_from[d], q, k, u)
                arrived(piece, UPX + u * 6 + q * 3 + d)
                send(piece, piece, UPC + u, to_core)

    def hidden_out(u, j):
        piece = h_buf.at[y, pl.ds(j * TC, TC), pl.ds(u * HALF, HALF)]
        for d in (1, 2, 0):
            send(piece, piece, HY + j, y_to[d], S_L)

    def hidden_half(u, order):
        arrived(up_buf.at[pl.ds(0, D // 2), pl.ds(u * HALF, HALF)], UPC + u)
        units = pl.ds(u * HALF, HALF)
        for part in range(2):
            at = pl.ds(part * TOK // 2, TOK // 2)
            pre = jnp.dot(nrm[at, :], up_buf[:, units], preferred_element_type=F32)
            pre = jnp.maximum(pre, 0.0)
            h_buf[y, at, units] = (pre * pre).astype(BF16)
            for uu, j in order[part]:
                hidden_out(uu, j)

    dt_over_core(0)
    up_to_core(0)
    arrived(dn_piece(og, x, k), DNG)
    dt_other = dn_buf[:, dn_cols(og, x, k)].astype(F32).T.astype(BF16)
    for h in range(2):
        dt_send[1, h] = dt_other[h * 64 : (h + 1) * 64]
    dt_over_y(1)

    hidden_half(0, (((0, 0), (0, 1)), ((0, 2),)))

    dt_over_x(1)
    up_to_core(1)
    hidden_half(1, (((1, 0), (1, 1)), ((1, 2), (0, 3), (1, 3))))

    dn_over_x(1)

    dt_over_core(1)

    @pl.when(jnp.logical_not(owner))
    def _():
        arrived(dt_buf, DTC)

    def times_hidden(first, j):
        rows_at = pl.ds(pl.multiple_of(first, 256), 256)
        total = jnp.zeros((256, TC), F32)
        for yy in range(4):
            total += lax.dot_general(
                dt_buf[yy, rows_at, :], h_buf[yy, pl.ds(j * TC, TC), :],
                (((1,), (1,)), ((), ())), preferred_element_type=F32,
            )
        return total

    def aligned(start, size):
        return pl.ds(pl.multiple_of(start, 64), size)

    def second_matmul(j):
        arrived(h_buf.at[pl.ds(0, 3), pl.ds(0, TC), :], HY + j)
        s1[j] = times_hidden((1 - b0) * 256, j).astype(BF16)
        send(s1.at[j], r1.at[j], RS + 3 * j, to_z1, S_L)
        k1[j] = times_hidden(b0 * 256, j)

    def halve(j):
        arrived(r1.at[j], RS + 3 * j)
        out, keep = aligned((1 - b1) * 128, 128), aligned(b1 * 128, 128)
        s2[j] = (k1[j, out, :] + r1[j, out, :].astype(F32)).astype(BF16)
        send(s2.at[j], r2.at[j], RS + 3 * j + 1, to_z2, S_L)
        k2[j] = k1[j, keep, :] + r1[j, keep, :].astype(F32)

    def halve_and_send(j):
        arrived(r1.at[j], RS + 3 * j)
        half_place = b1 * 2 + b2
        for m in (6, 4, 2):
            to, at_place = z_mate(m)
            at = at_place % 4
            rows_at = aligned(at * 64, 64)
            sm[j, at] = (k1[j, rows_at, :] + r1[j, rows_at, :].astype(F32)).astype(BF16)
            send(sm.at[j, at], rm.at[j, half_place], RS + 3 * j + 1, to, S_L)
        keep = aligned(half_place * 64, 64)
        k3[j] = k1[j, keep, :] + r1[j, keep, :].astype(F32)

    def second_matmul_to_all(j):
        arrived(h_buf.at[pl.ds(0, 3), pl.ds(0, TC), :], HY + j)
        sd[pl.ds((1 - b0) * 4, 4)] = times_hidden((1 - b0) * 256, j).astype(BF16).reshape(4, 64, TC)
        for m in (7, 5, 3, 1):
            to, at = z_mate(m)
            send(sd.at[at], rd.at[place], RS + 3 * j, to, S_L)
        kd[...] = times_hidden(b0 * 256, j).reshape(4, 64, TC)
        for m in (6, 4, 2):
            to, at = z_mate(m)
            sd[at] = kd[at % 4].astype(BF16)
            send(sd.at[at], rd.at[place], RS + 3 * j, to, S_L)

    def next_step(j):
        if STEPS[j] == 3:
            halve(j)
        elif STEPS[j] == 2:
            halve_and_send(j)

    for j in range(NT):
        if STEPS[j] == 1:
            second_matmul_to_all(j)
        else:
            second_matmul(j)
        if j >= 2:
            next_step(j - 2)
    next_step(NT - 2)
    next_step(NT - 1)
    for j in [j for j in range(NT) if STEPS[j] == 3]:
        arrived(r2.at[j], RS + 3 * j + 1)
        out, keep = aligned((1 - b2) * 64, 64), aligned(b2 * 64, 64)
        s3[j] = (k2[j, out, :] + r2[j, out, :].astype(F32)).astype(BF16)
        send(s3.at[j], r3.at[j], RS + 3 * j + 2, to_z4, S_L)
        k3[j] = k2[j, keep, :] + r2[j, keep, :].astype(F32)

    dn_over_core(0)
    dn_over_core(1)

    arrived(dn_buf.at[:, pl.ds(0, D // 2)], DNC)

    for j in range(NT):
        if STEPS[j] == 3:
            arrived(r3.at[j], RS + 3 * j + 2)
            total = k3[j] + r3[j].astype(F32)
        elif STEPS[j] == 2:
            arrived(rm.at[j, pl.ds(0, 3)], RS + 3 * j + 1)
            total = k3[j]
            for m in (2, 4, 6):
                total += rm[j, z_mate(m)[1] % 4].astype(F32)
        else:
            arrived(rd.at[pl.ds(0, 7)], RS + 3 * j)
            total = kd[place % 4]
            for m in range(1, 8):
                total += rd[z_mate(m)[1]].astype(F32)
        mix_ref[:, j * TC : (j + 1) * TC] = total.astype(BF16)

    all_left(S_W, (64 + 384 + 512 + 64 + 384 + 512) * KIB)
    all_left(S_L, (768 + NT * 112) * KIB)

    @pl.when(g == 1)
    def _():
        all_left(S_G, 64 * KIB)

    @pl.when(relays)
    def _():
        all_left(S_R, 128 * KIB)

    @pl.when(owner)
    def _():
        all_left(S_Y, 64 * KIB)
        all_left(S_X, 2 * 7 * 128 * KIB)

    @pl.when(jnp.logical_not(owner))
    def _():
        all_left(S_Y, 128 * KIB)


def write_out(up_ref, dn_ref, mix_ref, up_hbm, dn_hbm, mix_hbm, lsem):
    copies = [
        pltpu.make_async_copy(src, dst, lsem.at[i])
        for i, (src, dst) in enumerate(((up_ref, up_hbm), (dn_ref, dn_hbm), (mix_ref, mix_hbm)))
    ]
    for copy in copies:
        copy.start()
    for copy in copies:
        copy.wait()


def per_device(tokens, norm_gain, up_weight, down_weight):
    hbm = pl.BlockSpec(memory_space=pltpu.HBM)
    vmem = pl.BlockSpec(memory_space=pltpu.VMEM)
    up_block, down_block, mixed = pl.pallas_call(
        kernel,
        out_shape=(
            jax.ShapeDtypeStruct((D, UNITS), BF16),
            jax.ShapeDtypeStruct((UNITS, D), BF16),
            jax.ShapeDtypeStruct((64, TOK), BF16),
        ),
        in_specs=[hbm] * 4,
        out_specs=(vmem,) * 3,
        scratch_shapes=[
            pltpu.VMEM((1, 64), F32),
            pltpu.VMEM((64, 512), F32),
            pltpu.VMEM((256, 128), F32),
            pltpu.VMEM((2, 64, 256), BF16),
            pltpu.VMEM((2, 2, 64, 256), BF16),
            pltpu.VMEM((4, 512, 256), BF16),
            pltpu.VMEM((TOK, D), BF16),
            pltpu.VMEM((4, TOK, UNITS), BF16),
            pltpu.VMEM((NT, 256, TC), BF16),
            pltpu.VMEM((NT, 256, TC), BF16),
            pltpu.VMEM((NT, 256, TC), F32),
            pltpu.VMEM((NT, 128, TC), BF16),
            pltpu.VMEM((NT, 128, TC), BF16),
            pltpu.VMEM((NT, 128, TC), F32),
            pltpu.VMEM((NT, 64, TC), BF16),
            pltpu.VMEM((NT, 64, TC), BF16),
            pltpu.VMEM((NT, 64, TC), F32),
            pltpu.VMEM((NT, 4, 64, TC), BF16),
            pltpu.VMEM((NT, 4, 64, TC), BF16),
            pltpu.VMEM((8, 64, TC), BF16),
            pltpu.VMEM((8, 64, TC), BF16),
            pltpu.VMEM((4, 64, TC), F32),
            pltpu.SemaphoreType.DMA((N_SEND,)),
            pltpu.SemaphoreType.DMA((N_RECV,)),
            pltpu.SemaphoreType.DMA((4,)),
            pltpu.SemaphoreType.REGULAR,
        ],
        compiler_params=pltpu.CompilerParams(
            collective_id=0, has_side_effects=True, vmem_limit_bytes=16 * 1024 * 1024
        ),
        name="handoff",
    )(*(
        pltpu.with_memory_space_constraint(a, pltpu.HBM)
        for a in (tokens, norm_gain.reshape(1, 64), up_weight, down_weight)
    ))
    results = (up_block, down_block, mixed)
    up_block, down_block, mixed = pl.pallas_call(
        write_out,
        out_shape=tuple(jax.ShapeDtypeStruct(a.shape, a.dtype) for a in results),
        in_specs=[vmem] * 3,
        out_specs=(hbm,) * 3,
        scratch_shapes=[pltpu.SemaphoreType.DMA((3,))],
        compiler_params=pltpu.CompilerParams(vmem_limit_bytes=8 * 1024 * 1024),
        name="write_out",
    )(*results)
    return up_block, down_block, mixed.T


def solution(mesh):
    in_specs = (P(("gr", "tp"), None), P("fs"), P("fs", ("gr", "tp")), P("fs", ("gr", "tp")))
    out_specs = (P(None, "fs"), P("fs", None), P(("gr", "tp"), "fs"))
    return jax.shard_map(
        per_device, mesh=mesh, in_specs=in_specs, out_specs=out_specs, check_vma=False
    )
```
